256 devices in a mesh: grp: 2 (over y), ep: 64 (over z, x), tp: 2 (over core).
Axes of the slice: x: 4, y: 2, z: 16, core: 2. Of those that a mesh axis runs over, the one named last changes fastest.
The devices are a block of a 4x16x16 slice.
Arguments:
- hidden_state: bfloat16 [8192, 1024], P(('grp', 'ep'), 'tp'), parts along dimension 0, may hold values from -6 to 6
- expert_ids: int32 [8192, 4], P(('grp', 'ep')), parts along dimension 0, may hold values from 0 to 63, all different within a row; in each aligned block of 64 rows (0 to 63, 64 to 127, ...) at most 8 rows name the same one
- route_weight: float32 [8192, 4], P(('grp', 'ep')), parts along dimension 0, may hold values from 0.1 to 1
- gate_matrix: bfloat16 [64, 1024, 2048], P('ep', None, 'tp'), may hold values from -0.1875 to 0.1875
- up_matrix: bfloat16 [64, 1024, 2048], P('ep', None, 'tp'), may hold values from -0.1875 to 0.1875
- down_matrix: bfloat16 [64, 2048, 1024], P('ep', 'tp'), may hold values from -2 to 2
- norm_gain: float32 [1024], P('tp'), may hold values from 0.1 to 1.9
Outputs:
- normed_out: bfloat16 [8192, 1024], P(('grp', 'ep'), 'tp'), parts along dimension 0
The draws below stay inside these ranges and needn't reach their ends.
There are 2 independent parts, one for each index of `grp`. The reference program is written for one: setup_inputs(seed, part) draws one part's arguments, and reference() takes and returns one part's arrays. A program takes and returns all parts, laid end to end along the dimension named above; an argument that names none is the same for every part. Nothing has to cross between parts.
Inputs may be any that keep to these rules, and one draw needn't show every extreme that they name: `expert_ids`: each row names 4 different experts. Within the rows of one index of ep (aligned blocks of 64 rows) no expert is named by more than 8 rows, and in some blocks one expert is named by exactly 8 rows. Every expert is named by some row.
All inputs are finite; a program needn't handle non-finite values.
Results may differ from the reference program's by a relative error of at most 0.0065.
Values may be sent and summed in bfloat16 or wider, within the bound.
No kernel may reach another device: no remote copies, remote signals or barrier semaphores. Data moves between devices by JAX's collectives and lax.ppermute only.
A program may use at most 64 MiB of HBM per device.

```python
import math
import jax
import jax.numpy as jnp
import numpy as np
from jax import lax

D = 1024
FF = 2048
TOPK = 4
TOK_DEV = 64
EXPERTS = 64
TOKENS = 4096
CAP = 8
N_EP = 64
N_TP = 2


def draw_down_matrix(key, part):
    noise_key = jax.random.fold_in(key, 11)
    scale_key = jax.random.fold_in(key, 23)
    column = jnp.arange(D, dtype=jnp.float32) / D
    jitter = jax.random.uniform(scale_key, (D,), jnp.float32, -0.35, 0.35)
    base = jnp.clip(jax.random.normal(noise_key, (EXPERTS, FF, D), jnp.float32), -6.0, 6.0)
    column_scale = jnp.exp(math.log(10.0) * column + jitter)
    values = base * column_scale[None, None, :] * FF ** (-0.5)
    return jnp.clip(values, -2.0, 2.0).astype(jnp.bfloat16)


def block_scale(key, shape, cuts, low, top_value):
    factor_of = 1.0
    for axis_at, shards_of in cuts:
        heights = jax.random.uniform(jax.random.fold_in(jax.random.fold_in(key, 6), axis_at), (shards_of,), jnp.float32, low / len(cuts), top_value / len(cuts))
        factor_of = factor_of * jnp.repeat(jnp.exp(heights), shape[axis_at] // shards_of).reshape((-1,) + (1,) * (len(shape) - 1 - axis_at))
    return factor_of


def deal_out(key, own, number, rows, number_of, top, bound, slope):
    sequence = jax.random.permutation(key, number_of)
    packed, ordinary = load_shares(number_of, rows * top, bound, slope, True), load_shares(number_of, rows * top, bound, slope, False)
    places = jnp.arange(number_of)

    def named(sizes, offset_by):
        used = int((sizes > 0).sum())
        fixed = max(1, used // 4)
        moved = fixed + (places - fixed + offset_by * (used - fixed)) % max(1, number_of - fixed)
        return jnp.zeros((number_of,), jnp.int32).at[sequence[jnp.where(places < fixed, places, moved)]].set(jnp.asarray(sizes, jnp.int32))

    sizes = jnp.where(number % 4 == 0, named(packed, number // 4), named(ordinary, number - number // 4 - 1))
    mixed = jax.random.permutation(jax.random.fold_in(own, 3), number_of)
    donor, taker = mixed[0:number_of // 2 * 2:2], mixed[1:number_of // 2 * 2:2]
    room = jnp.minimum(sizes[donor] - 1, bound - sizes[taker]) // 2
    room = jnp.where((donor == sequence[0]) | (taker == sequence[0]) | (sizes[taker] == 0), 0, jnp.maximum(room, 0))
    moved = jax.random.randint(jax.random.fold_in(own, 4), (number_of // 2,), 0, 1 << 20) % (room + 1)
    sizes = sizes.at[donor].add(-moved).at[taker].add(moved)
    members = jnp.searchsorted(jnp.cumsum(sizes), jnp.arange(rows * top), side="right").astype(jnp.int32)
    grid = members.reshape(top, rows).T
    grid = grid[jax.random.permutation(jax.random.fold_in(own, 1), rows)]
    offset_by = jax.random.randint(jax.random.fold_in(own, 2), (rows, 1), 0, top)
    return jnp.take_along_axis(grid, (jnp.arange(top)[None, :] + offset_by) % top, axis=1)


def load_shares(number_of, total, reach, slope, full):
    weights = [(1 << 20) // math.isqrt(standing ** slope) + 1 for standing in range(1, number_of + 1)]
    largest = reach if full else min(reach, max(-(-total // number_of), total * weights[0] // sum(weights)))
    least = 1 if total - largest >= number_of - 1 else 0
    counts, rest = [largest] + [least] * (number_of - 1), total - largest - least * (number_of - 1)
    while rest > 0:
        candidates = [i for i in range(1, number_of) if counts[i] < largest] or [i for i in range(1, number_of) if counts[i] < reach]
        whole, budget = sum([weights[i] for i in candidates]), rest
        for i in candidates:
            extra = min(reach - counts[i], max(1, budget * weights[i] // whole), rest)
            counts[i] = counts[i] + extra
            rest = rest - extra
    return np.array(counts)


def centred(rng, extent, width, bound, pieces=(), kind=jnp.bfloat16):
    array = jax.random.normal(rng, extent, jnp.float32) * width
    if len(pieces) > 0:
        array = block_scale(rng, extent, pieces, -0.22, 0.18) * array
    return jnp.clip(array, min=-bound, max=bound).astype(kind)


def setup_inputs(seed: int = 0, part: int = 0) -> dict:
    seeds = jax.random.split(jax.random.key(seed), 8)
    own_keys = jax.random.split(jax.random.fold_in(seeds[7], part), 8)
    hidden_state = centred(own_keys[0], (TOKENS, D), 1.0, 6.0, ((0, 64), (1, 2)))
    expert_ids_keys = jax.random.split(jax.random.fold_in(own_keys[1], 1), TOKENS // TOK_DEV)
    expert_ids_turns = jax.random.permutation(jax.random.fold_in(own_keys[1], 3), TOKENS // TOK_DEV)
    expert_ids = jax.vmap(lambda own, number: deal_out(jax.random.fold_in(own_keys[1], 2), own, number, TOK_DEV, EXPERTS, TOPK, CAP, 2))(expert_ids_keys, expert_ids_turns).reshape((TOKENS, TOPK))
    route_weight = jnp.clip(jnp.exp(math.log(1.0) - 2.3025851 * jax.random.uniform(own_keys[2], (TOKENS, TOPK), jnp.float32) ** block_scale(own_keys[2], (TOKENS, TOPK), ((0, 64),), -0.2, 0.2)), 0.1, 1.0)
    gate_matrix = centred(seeds[3], (EXPERTS, D, FF), D ** -0.5, 0.1875, ((0, 64), (2, 2)))
    up_matrix = centred(seeds[4], (EXPERTS, D, FF), D ** -0.5, 0.1875, ((0, 64), (2, 2)))
    down_matrix = draw_down_matrix(jax.random.fold_in(seeds[7], 71), part)
    norm_gain = jnp.clip(1.0 + 0.18 * jax.random.normal(seeds[6], (D,), jnp.float32), 0.1, 1.9)
    return {"hidden_state": hidden_state, "expert_ids": expert_ids, "route_weight": route_weight, "gate_matrix": gate_matrix, "up_matrix": up_matrix, "down_matrix": down_matrix, "norm_gain": norm_gain}


def slot_ranks(expert_ids):
    blocks = expert_ids.reshape(N_EP, TOK_DEV * TOPK)
    onehot = (blocks[:, :, None] == jnp.arange(EXPERTS, dtype=jnp.int32)[None, None, :]).astype(jnp.int32)
    earlier = jnp.cumsum(onehot, axis=1) - onehot
    return lax.optimization_barrier(jnp.sum(earlier * onehot, axis=2)).astype(jnp.int32).reshape(TOKENS, TOPK)

def reference(hidden_state, expert_ids, route_weight, gate_matrix, up_matrix, down_matrix, norm_gain):
    slot_rank = slot_ranks(expert_ids)
    block_index = (jnp.arange(TOKENS, dtype=jnp.int32) // TOK_DEV)[:, None]
    slot_index = (block_index * CAP + slot_rank).astype(jnp.int32)
    token_ids = jnp.broadcast_to(jnp.arange(TOKENS, dtype=jnp.int32)[:, None], (TOKENS, TOPK))
    slot_table = jnp.zeros((EXPERTS, N_EP * CAP), jnp.int32).at[expert_ids, slot_index].set(token_ids)
    half_width = FF // N_TP

    def one_expert(operands):
        row_index, gate_block, up_block, down_block = operands
        token_rows = hidden_state[row_index]
        gate_pre = jnp.dot(token_rows, gate_block, preferred_element_type=jnp.float32)
        up_pre = jnp.dot(token_rows, up_block, preferred_element_type=jnp.float32)
        activated = (jax.nn.silu(gate_pre) * up_pre).astype(jnp.bfloat16)
        summed_rows = jnp.zeros((token_rows.shape[0], D), jnp.float32)
        for segment in range(N_TP):
            partial_value = jnp.dot(activated[:, segment * half_width:(segment + 1) * half_width], down_block[segment * half_width:(segment + 1) * half_width], preferred_element_type=jnp.float32).astype(jnp.bfloat16)
            partial_value = lax.optimization_barrier(partial_value)
            summed_rows = summed_rows + partial_value.astype(jnp.float32)
        return summed_rows.astype(jnp.bfloat16)
    outputs = lax.map(one_expert, (slot_table, gate_matrix, up_matrix, down_matrix))
    picked = outputs[expert_ids, slot_index]
    combined = lax.optimization_barrier(jnp.sum(route_weight[:, :, None].astype(jnp.float32) * picked.astype(jnp.float32), axis=1))
    mean_square = lax.optimization_barrier(jnp.mean(combined * combined, axis=1, keepdims=True))
    return (combined * lax.rsqrt(mean_square + 1e-05) * norm_gain).astype(jnp.bfloat16)
```

```python
import functools

import jax
import jax.numpy as jnp
from jax import lax
from jax.experimental import pallas as pl
from jax.experimental.pallas import tpu as pltpu
from jax.sharding import PartitionSpec as P

norm_eps = 1e-05
f32, bf16, i32 = jnp.float32, jnp.bfloat16, jnp.int32


def dot(a, b, dims=((1,), (0,))):
    return lax.dot_general(a, b, (dims, ((), ())), preferred_element_type=f32)


def iota(shape, dim):
    return lax.broadcasted_iota(i32, shape, dim)


def slot_ranks(ids, expert_count):
    rows, top = ids.shape
    lanes = iota((rows, expert_count), 1)
    named = ids[:, 0:1] == lanes
    for k in range(1, top):
        named = named | (ids[:, k : k + 1] == lanes)
    named = jnp.where(named, 1.0, 0.0)
    earlier = jnp.where(iota((rows, rows), 1) < iota((rows, rows), 0), 1.0, 0.0)
    return named, dot(earlier.astype(bf16), named.astype(bf16))


def pack_body(ids_ref, hidden_ref, out_ref, *, expert_count, capacity):
    named, rank = slot_ranks(ids_ref[...], expert_count)
    code = jnp.where(named > 0, rank, -1.0).astype(bf16)
    slots = expert_count * capacity
    spread = iota((slots, expert_count), 0) // capacity == iota((slots, expert_count), 1)
    spread = jnp.where(spread, 1.0, 0.0).astype(bf16)
    wanted = dot(spread, code, ((1,), (1,)))
    own = (iota(wanted.shape, 0) % capacity).astype(f32)
    placing = jnp.where(wanted == own, 1.0, 0.0).astype(bf16)
    out_ref[...] = dot(placing, hidden_ref[...]).astype(bf16)


def pack(ids, hidden, expert_count, capacity):
    body = functools.partial(pack_body, expert_count=expert_count, capacity=capacity)
    return pl.pallas_call(
        body,
        out_shape=jax.ShapeDtypeStruct((expert_count * capacity, hidden.shape[1]), bf16),
        name="pack",
    )(ids, hidden)


def hidden_body(tp_ref, own_ref, other_ref, gate_ref, up_ref, down_ref, act_ref, send_ref, acc_ref):
    step = pl.program_id(0)
    half = own_ref.shape[1]
    mine = pl.multiple_of(tp_ref[0] * half, half)
    theirs = pl.multiple_of((1 - tp_ref[0]) * half, half)
    own, other = own_ref[...], other_ref[...]
    gate = dot(own, gate_ref[0, pl.ds(mine, half), :]) + dot(other, gate_ref[0, pl.ds(theirs, half), :])
    up = dot(own, up_ref[0, pl.ds(mine, half), :]) + dot(other, up_ref[0, pl.ds(theirs, half), :])
    act = (gate / (1.0 + jnp.exp(-gate)) * up).astype(bf16)
    act_ref[...] = act
    part = dot(act, down_ref[0])

    @pl.when(step == 0)
    def _():
        acc_ref[...] = part

    @pl.when(step > 0)
    def _():
        acc_ref[...] += part

    @pl.when(step == pl.num_programs(0) - 1)
    def _():
        send_ref[...] = acc_ref[...].astype(bf16)


def hidden_part(tp, own, other, gate, up, down, tile=256):
    rows, half = own.shape
    width, units = gate.shape[1:]
    whole = pl.BlockSpec((rows, half), lambda j, t: (0, 0))
    return pl.pallas_call(
        hidden_body,
        grid_spec=pltpu.PrefetchScalarGridSpec(
            num_scalar_prefetch=1,
            grid=(units // tile,),
            in_specs=[
                whole,
                whole,
                pl.BlockSpec((1, width, tile), lambda j, t: (0, 0, j)),
                pl.BlockSpec((1, width, tile), lambda j, t: (0, 0, j)),
                pl.BlockSpec((1, tile, half), lambda j, t: (0, j, 1 - t[0])),
            ],
            out_specs=[pl.BlockSpec((rows, tile), lambda j, t: (0, j)), whole],
            scratch_shapes=[pltpu.VMEM((rows, half), f32)],
        ),
        out_shape=[jax.ShapeDtypeStruct((rows, units), bf16), jax.ShapeDtypeStruct((rows, half), bf16)],
        cost_estimate=pl.CostEstimate(
            flops=2 * rows * units * (2 * width + half), bytes_accessed=2 * units * (2 * width + half), transcendentals=rows * units
        ),
        name="hidden_part",
    )(tp, own, other, gate, up, down)


def keep_body(tp_ref, act_ref, down_ref, out_ref):
    out_ref[...] = dot(act_ref[...], down_ref[0]).astype(bf16)


def keep_part(tp, act, down, half):
    rows, units = act.shape
    return pl.pallas_call(
        keep_body,
        grid_spec=pltpu.PrefetchScalarGridSpec(
            num_scalar_prefetch=1,
            grid=(1,),
            in_specs=[
                pl.BlockSpec((rows, units), lambda j, t: (0, 0)),
                pl.BlockSpec((1, units, half), lambda j, t: (0, 0, t[0])),
            ],
            out_specs=pl.BlockSpec((rows, half), lambda j, t: (0, 0)),
        ),
        out_shape=jax.ShapeDtypeStruct((rows, half), bf16),
        cost_estimate=pl.CostEstimate(flops=2 * rows * units * half, bytes_accessed=2 * units * half, transcendentals=0),
        name="keep_part",
    )(tp, act, down)


def combine_body(ids_ref, weight_ref, back_ref, out_ref, square_ref, *, expert_count, capacity):
    ids = ids_ref[...]
    rows, top = ids.shape
    _, rank = slot_ranks(ids, expert_count)
    lanes = iota((rows, expert_count), 1)
    places = iota((rows, expert_count * capacity), 1)
    weights = jnp.zeros(places.shape, f32)
    for k in range(top):
        column = ids[:, k : k + 1]
        at = jnp.sum(jnp.where(column == lanes, rank, 0.0), axis=1, keepdims=True).astype(i32)
        weights += jnp.where(column * capacity + at == places, weight_ref[:, k : k + 1], 0.0)
    high = weights.astype(bf16)
    low = (weights - high.astype(f32)).astype(bf16)
    back = back_ref[...]
    combined = dot(high, back) + dot(low, back)
    out_ref[...] = combined
    square_ref[...] = jnp.broadcast_to(jnp.sum(combined * combined, axis=1, keepdims=True), square_ref.shape)


def combine(ids, weights, back, expert_count, capacity):
    rows = ids.shape[0]
    body = functools.partial(combine_body, expert_count=expert_count, capacity=capacity)
    return pl.pallas_call(
        body,
        out_shape=[jax.ShapeDtypeStruct((rows, back.shape[1]), f32), jax.ShapeDtypeStruct((rows, 128), f32)],
        name="combine",
    )(ids, weights, back)


def shards(hidden_state, expert_ids, route_weight, gate_matrix, up_matrix, down_matrix, norm_gain):
    tok_count, top_count = expert_ids.shape
    half = hidden_state.shape[1]
    experts = lax.axis_size("ep")
    capacity = max(2, 2 * tok_count * top_count // experts)
    tp = lax.axis_index("tp").reshape(1)
    swap = lambda a: lax.ppermute(a, "tp", [(0, 1), (1, 0)])
    exchange = lambda a: lax.all_to_all(a.reshape(experts, capacity, half), "ep", 0, 0, tiled=True).reshape(
        experts * capacity, half
    )
    own = exchange(pack(expert_ids, hidden_state, experts, capacity))
    act, send = hidden_part(tp, own, swap(own), gate_matrix, up_matrix, down_matrix)
    got = swap(send)
    kept = keep_part(tp, act, down_matrix, half)
    answers = (kept.astype(f32) + got.astype(f32)).astype(bf16)
    combined, squares = combine(expert_ids, route_weight, exchange(answers), experts, capacity)
    total = (squares + swap(squares))[:, :1]
    width = half * lax.axis_size("tp")
    return (combined * lax.rsqrt(total / width + norm_eps) * norm_gain).astype(bf16)


def solution(mesh):
    placed = (
        P(("grp", "ep"), "tp"),
        P(("grp", "ep"), None),
        P(("grp", "ep"), None),
        P("ep", None, "tp"),
        P("ep", None, "tp"),
        P("ep", "tp", None),
        P("tp"),
    )
    return jax.shard_map(
        shards, mesh=mesh, in_specs=placed, out_specs=P(("grp", "ep"), "tp"), check_vma=False
    )
```

```python
import functools

import jax
import jax.numpy as jnp
from jax import lax
from jax.experimental import pallas as pl
from jax.experimental.pallas import tpu as pltpu
from jax.sharding import PartitionSpec as P

norm_eps = 1e-05
f32, bf16, i32 = jnp.float32, jnp.bfloat16, jnp.int32
VMEM = pl.BlockSpec(memory_space=pltpu.VMEM)
SMEM = pl.BlockSpec(memory_space=pltpu.SMEM)


def call(body, name, mib, in_specs, out_shape, scratch=(), cost=None):
    return pl.pallas_call(
        body,
        in_specs=in_specs,
        out_specs=jax.tree.map(lambda _: VMEM, out_shape),
        out_shape=out_shape,
        scratch_shapes=scratch,
        cost_estimate=cost,
        compiler_params=pltpu.CompilerParams(vmem_limit_bytes=mib << 20),
        name=name,
    )


def dot(a, b, dims=((1,), (0,))):
    return lax.dot_general(a, b, (dims, ((), ())), preferred_element_type=f32)


def iota(shape, dim):
    return lax.broadcasted_iota(i32, shape, dim)


def slot_ranks(ids, expert_count):
    top, rows = ids.shape
    experts = iota((expert_count, rows), 0)
    named = ids[0:1] == experts
    for k in range(1, top):
        named = named | (ids[k : k + 1] == experts)
    named = jnp.where(named, 1.0, 0.0)
    earlier = jnp.where(iota((rows, rows), 0) < iota((rows, rows), 1), 1.0, 0.0)
    return named, dot(named.astype(bf16), earlier.astype(bf16))


def pack_body(ids_ref, hidden_ref, out_ref, *, expert_count, capacity):
    named, rank = slot_ranks(ids_ref[...], expert_count)
    code = jnp.where(named > 0, rank, -1.0).astype(bf16)
    slots = expert_count * capacity
    spread = iota((slots, expert_count), 0) // capacity == iota((slots, expert_count), 1)
    spread = jnp.where(spread, 1.0, 0.0).astype(bf16)
    wanted = dot(spread, code)
    own = (iota(wanted.shape, 0) % capacity).astype(f32)
    placing = jnp.where(wanted == own, 1.0, 0.0).astype(bf16)
    out_ref[...] = dot(placing, hidden_ref[...]).astype(bf16)


def pack(ids, hidden, expert_count, capacity):
    body = functools.partial(pack_body, expert_count=expert_count, capacity=capacity)
    out = jax.ShapeDtypeStruct((expert_count * capacity, hidden.shape[1]), bf16)
    return call(body, "pack", 4, [VMEM] * 2, out)(ids, hidden)


def hidden_body(tp_ref, own_ref, other_ref, gate_ref, up_ref, down_ref, act_ref, send_ref, *, tile):
    half = own_ref.shape[1]
    units = gate_ref.shape[2]
    mine = pl.multiple_of(tp_ref[0] * half, half)
    theirs = pl.multiple_of((1 - tp_ref[0]) * half, half)
    own, other = own_ref[...], other_ref[...]
    for start in range(0, units, tile):
        at = slice(start, start + tile)
        gate = dot(own, gate_ref[0, pl.ds(mine, half), at]) + dot(other, gate_ref[0, pl.ds(theirs, half), at])
        up = dot(own, up_ref[0, pl.ds(mine, half), at]) + dot(other, up_ref[0, pl.ds(theirs, half), at])
        act_ref[:, at] = (gate / (1.0 + jnp.exp(-gate)) * up).astype(bf16)
    send_ref[...] = dot(act_ref[...], down_ref[0, :, pl.ds(theirs, half)]).astype(bf16)


def hidden_part(tp, own, other, gate, up, down, tile=256):
    rows, half = own.shape
    width, units = gate.shape[1:]
    cost = pl.CostEstimate(
        flops=2 * rows * units * (2 * width + half), bytes_accessed=2 * units * (2 * width + half), transcendentals=rows * units
    )
    out = [jax.ShapeDtypeStruct((rows, units), bf16), jax.ShapeDtypeStruct((rows, half), bf16)]
    body = functools.partial(hidden_body, tile=tile)
    return call(body, "hidden_part", 16, [SMEM] + [VMEM] * 5, out, cost=cost)(tp, own, other, gate, up, down)


def keep_body(tp_ref, act_ref, down_ref, out_ref):
    half = out_ref.shape[1]
    mine = pl.multiple_of(tp_ref[0] * half, half)
    out_ref[...] = dot(act_ref[...], down_ref[0, :, pl.ds(mine, half)]).astype(bf16)


def keep_part(tp, act, down, half):
    rows, units = act.shape
    cost = pl.CostEstimate(flops=2 * rows * units * half, bytes_accessed=2 * units * half, transcendentals=0)
    out = jax.ShapeDtypeStruct((rows, half), bf16)
    return call(keep_body, "keep_part", 8, [SMEM] + [VMEM] * 2, out, cost=cost)(tp, act, down)


def combine_body(ids_ref, weight_ref, back_ref, out_ref, square_ref, *, expert_count, capacity):
    ids = ids_ref[...]
    top, rows = ids.shape
    _, rank = slot_ranks(ids, expert_count)
    experts = iota((expert_count, rows), 0)
    places = iota((expert_count * capacity, rows), 0)
    weights = jnp.zeros(places.shape, f32)
    for k in range(top):
        row = ids[k : k + 1]
        at = jnp.sum(jnp.where(row == experts, rank, 0.0), axis=0, keepdims=True).astype(i32)
        weights += jnp.where(row * capacity + at == places, weight_ref[k : k + 1], 0.0)
    high = weights.astype(bf16)
    low = (weights - high.astype(f32)).astype(bf16)
    back = back_ref[...]
    over = ((0,), (0,))
    combined = dot(high, back, over) + dot(low, back, over)
    out_ref[...] = combined
    square_ref[...] = jnp.broadcast_to(jnp.sum(combined * combined, axis=1, keepdims=True), square_ref.shape)


def combine(ids, weights, back, expert_count, capacity):
    rows = ids.shape[1]
    body = functools.partial(combine_body, expert_count=expert_count, capacity=capacity)
    out = [jax.ShapeDtypeStruct((rows, back.shape[1]), f32), jax.ShapeDtypeStruct((rows, 128), f32)]
    return call(body, "combine", 4, [VMEM] * 3, out)(ids, weights, back)


def norm_body(combined_ref, square_ref, other_ref, gain_ref, out_ref, *, width):
    total = (square_ref[...] + other_ref[...])[:, 0:1]
    out_ref[...] = (combined_ref[...] * lax.rsqrt(total / width + norm_eps) * gain_ref[...]).astype(bf16)


def norm(combined, squares, others, gain, width):
    body = functools.partial(norm_body, width=width)
    out = jax.ShapeDtypeStruct(combined.shape, bf16)
    return call(body, "norm", 4, [VMEM] * 4, out)(combined, squares, others, gain.reshape(1, -1))


def shards(hidden_state, expert_ids, route_weight, gate_matrix, up_matrix, down_matrix, norm_gain):
    tok_count, top_count = expert_ids.shape
    half = hidden_state.shape[1]
    experts = lax.axis_size("ep")
    capacity = max(2, 2 * tok_count * top_count // experts)
    tp = lax.axis_index("tp").reshape(1)
    ids, weights = expert_ids.T, route_weight.T
    swap = lambda a: lax.ppermute(a, "tp", [(0, 1), (1, 0)])
    exchange = lambda a: lax.all_to_all(a.reshape(experts, capacity, half), "ep", 0, 0, tiled=True).reshape(
        experts * capacity, half
    )
    own = exchange(pack(ids, hidden_state, experts, capacity))
    act, send = hidden_part(tp, own, swap(own), gate_matrix, up_matrix, down_matrix)
    got = swap(send)
    kept = keep_part(tp, act, down_matrix, half)
    answers = (kept.astype(f32) + got.astype(f32)).astype(bf16)
    combined, squares = combine(ids, weights, exchange(answers), experts, capacity)
    return norm(combined, squares, swap(squares), norm_gain, half * lax.axis_size("tp"))


def solution(mesh):
    placed = (
        P(("grp", "ep"), "tp"),
        P(("grp", "ep"), None),
        P(("grp", "ep"), None),
        P("ep", None, "tp"),
        P("ep", None, "tp"),
        P("ep", "tp", None),
        P("tp"),
    )
    return jax.shard_map(
        shards, mesh=mesh, in_specs=placed, out_specs=P(("grp", "ep"), "tp"), check_vma=False
    )
```

```python
import functools

import jax
import jax.numpy as jnp
from jax import lax
from jax.experimental import pallas as pl
from jax.experimental.pallas import tpu as pltpu
from jax.sharding import PartitionSpec as P

norm_eps = 1e-05
f32, bf16, i32 = jnp.float32, jnp.bfloat16, jnp.int32
VMEM = pl.BlockSpec(memory_space=pltpu.VMEM)
SMEM = pl.BlockSpec(memory_space=pltpu.SMEM)
HBM = pl.BlockSpec(memory_space=pltpu.HBM)


def call(body, name, mib, in_specs, out_shape, scratch=(), cost=None):
    return pl.pallas_call(
        body,
        in_specs=in_specs,
        out_specs=jax.tree.map(lambda _: VMEM, out_shape),
        out_shape=out_shape,
        scratch_shapes=scratch,
        cost_estimate=cost,
        compiler_params=pltpu.CompilerParams(vmem_limit_bytes=mib << 20),
        name=name,
    )


def dot(a, b, dims=((1,), (0,))):
    return lax.dot_general(a, b, (dims, ((), ())), preferred_element_type=f32)


def in_hbm(array):
    return pltpu.with_memory_space_constraint(array, pltpu.HBM)


def iota(shape, dim):
    return lax.broadcasted_iota(i32, shape, dim)


def slot_ranks(ids, expert_count):
    top, rows = ids.shape
    experts = iota((expert_count, rows), 0)
    named = ids[0:1] == experts
    for k in range(1, top):
        named = named | (ids[k : k + 1] == experts)
    named = jnp.where(named, 1.0, 0.0)
    earlier = jnp.where(iota((rows, rows), 0) < iota((rows, rows), 1), 1.0, 0.0)
    return named, dot(named.astype(bf16), earlier.astype(bf16))


def pack_body(ids_hbm, hidden_hbm, out_ref, ids_ref, hidden_ref, sems, *, expert_count, capacity):
    ids_copy = pltpu.make_async_copy(ids_hbm, ids_ref, sems.at[0])
    hidden_copy = pltpu.make_async_copy(hidden_hbm, hidden_ref, sems.at[1])
    ids_copy.start()
    hidden_copy.start()
    slots = expert_count * capacity
    spread = iota((slots, expert_count), 0) // capacity == iota((slots, expert_count), 1)
    spread = jnp.where(spread, 1.0, 0.0).astype(bf16)
    ids_copy.wait()
    named, rank = slot_ranks(ids_ref[...], expert_count)
    code = jnp.where(named > 0, rank, -1.0).astype(bf16)
    wanted = dot(spread, code)
    own = (iota(wanted.shape, 0) % capacity).astype(f32)
    placing = jnp.where(wanted == own, 1.0, 0.0).astype(bf16)
    hidden_copy.wait()
    out_ref[...] = dot(placing, hidden_ref[...]).astype(bf16)


def pack(ids, hidden, expert_count, capacity):
    body = functools.partial(pack_body, expert_count=expert_count, capacity=capacity)
    out = jax.ShapeDtypeStruct((expert_count * capacity, hidden.shape[1]), bf16)
    scratch = [pltpu.VMEM(ids.shape, i32), pltpu.VMEM(hidden.shape, bf16), pltpu.SemaphoreType.DMA((2,))]
    return call(body, "pack", 4, [HBM] * 2, out, scratch)(in_hbm(ids), in_hbm(hidden))


def own_body(tp_ref, own_ref, gate_hbm, up_hbm, down_hbm, gate_out, up_out, gate_rest, up_rest, down_send, down_keep, gate_ref, up_ref, sems, *, tile):
    half = own_ref.shape[1]
    units = gate_ref.shape[1]
    steps = units // tile
    mine = pl.ds(pl.multiple_of(tp_ref[0] * half, half), half)
    theirs = pl.ds(pl.multiple_of((1 - tp_ref[0]) * half, half), half)
    copies = []
    for j in range(steps):
        at = slice(j * tile, (j + 1) * tile)
        for source, target in ((gate_hbm, gate_ref), (up_hbm, up_ref)):
            copies.append(pltpu.make_async_copy(source.at[0, mine, at], target.at[:, at], sems.at[len(copies)]))
    for source, target in (
        (gate_hbm.at[0, theirs, :], gate_rest),
        (up_hbm.at[0, theirs, :], up_rest),
        (down_hbm.at[0, :, theirs], down_send),
        (down_hbm.at[0, :, mine], down_keep),
    ):
        copies.append(pltpu.make_async_copy(source, target, sems.at[len(copies)]))
    for copy in copies:
        copy.start()
    own = own_ref[...]
    for j in range(steps):
        at = slice(j * tile, (j + 1) * tile)
        copies[2 * j].wait()
        gate_out[:, at] = dot(own, gate_ref[:, at])
        copies[2 * j + 1].wait()
        up_out[:, at] = dot(own, up_ref[:, at])
    for copy in copies[2 * steps :]:
        copy.wait()


def own_part(tp, own, gate, up, down, tile=256):
    rows, half = own.shape
    units = gate.shape[2]
    cost = pl.CostEstimate(flops=4 * rows * units * half, bytes_accessed=6 * units * units, transcendentals=0)
    shape = jax.ShapeDtypeStruct
    out = [shape((rows, units), f32)] * 2 + [shape((half, units), bf16)] * 2 + [shape((units, half), bf16)] * 2
    scratch = [pltpu.VMEM((half, units), bf16)] * 2 + [pltpu.SemaphoreType.DMA((2 * (units // tile) + 4,))]
    body = functools.partial(own_body, tile=tile)
    return call(body, "own_part", 16, [SMEM, VMEM] + [HBM] * 3, out, scratch, cost)(tp, own, *map(in_hbm, (gate, up, down)))


def hidden_body(other_ref, gate_in, up_in, gate_ref, up_ref, down_ref, act_ref, send_ref, *, tile):
    other = other_ref[...]
    for start in range(0, gate_ref.shape[1], tile):
        at = slice(start, start + tile)
        gate = gate_in[:, at] + dot(other, gate_ref[:, at])
        up = up_in[:, at] + dot(other, up_ref[:, at])
        act_ref[:, at] = (gate / (1.0 + jnp.exp(-gate)) * up).astype(bf16)
    send_ref[...] = dot(act_ref[...], down_ref[...]).astype(bf16)


def hidden_part(other, gate_in, up_in, gate_rest, up_rest, down_send, tile=256):
    rows, half = other.shape
    units = gate_rest.shape[1]
    cost = pl.CostEstimate(flops=6 * rows * units * half, bytes_accessed=6 * units * half, transcendentals=rows * units)
    out = [jax.ShapeDtypeStruct((rows, units), bf16), jax.ShapeDtypeStruct((rows, half), bf16)]
    body = functools.partial(hidden_body, tile=tile)
    return call(body, "hidden_part", 16, [VMEM] * 6, out, cost=cost)(other, gate_in, up_in, gate_rest, up_rest, down_send)


def keep_body(act_ref, down_ref, out_ref):
    out_ref[...] = dot(act_ref[...], down_ref[...]).astype(bf16)


def keep_part(act, down_keep):
    rows, units = act.shape
    half = down_keep.shape[1]
    cost = pl.CostEstimate(flops=2 * rows * units * half, bytes_accessed=2 * units * half, transcendentals=0)
    return call(keep_body, "keep_part", 8, [VMEM] * 2, jax.ShapeDtypeStruct((rows, half), bf16), cost=cost)(act, down_keep)


def combine_body(ids_ref, weight_ref, back_ref, out_ref, square_ref, *, expert_count, capacity):
    ids = ids_ref[...]
    top, rows = ids.shape
    _, rank = slot_ranks(ids, expert_count)
    experts = iota((expert_count, rows), 0)
    places = iota((expert_count * capacity, rows), 0)
    weights = jnp.zeros(places.shape, f32)
    for k in range(top):
        row = ids[k : k + 1]
        at = jnp.sum(jnp.where(row == experts, rank, 0.0), axis=0, keepdims=True).astype(i32)
        weights += jnp.where(row * capacity + at == places, weight_ref[k : k + 1], 0.0)
    high = weights.astype(bf16)
    low = (weights - high.astype(f32)).astype(bf16)
    back = back_ref[...]
    over = ((0,), (0,))
    combined = dot(high, back, over) + dot(low, back, over)
    out_ref[...] = combined
    square_ref[...] = jnp.broadcast_to(jnp.sum(combined * combined, axis=1, keepdims=True), square_ref.shape)


def combine(ids, weights, back, expert_count, capacity):
    rows = ids.shape[1]
    body = functools.partial(combine_body, expert_count=expert_count, capacity=capacity)
    out = [jax.ShapeDtypeStruct((rows, back.shape[1]), f32), jax.ShapeDtypeStruct((rows, 128), f32)]
    return call(body, "combine", 4, [VMEM] * 3, out)(ids, weights, back)


def norm_body(combined_ref, square_ref, other_ref, gain_ref, out_ref, *, width):
    total = (square_ref[...] + other_ref[...])[:, 0:1]
    out_ref[...] = (combined_ref[...] * lax.rsqrt(total / width + norm_eps) * gain_ref[...]).astype(bf16)


def norm(combined, squares, others, gain, width):
    body = functools.partial(norm_body, width=width)
    out = jax.ShapeDtypeStruct(combined.shape, bf16)
    return call(body, "norm", 4, [VMEM] * 4, out)(combined, squares, others, gain.reshape(1, -1))


def shards(hidden_state, expert_ids, route_weight, gate_matrix, up_matrix, down_matrix, norm_gain):
    tok_count, top_count = expert_ids.shape
    half = hidden_state.shape[1]
    experts = lax.axis_size("ep")
    capacity = max(2, 2 * tok_count * top_count // experts)
    tp = lax.axis_index("tp").reshape(1)
    ids, weights = expert_ids.T, route_weight.T
    swap = lambda a: lax.ppermute(a, "tp", [(0, 1), (1, 0)])
    exchange = lambda a: lax.all_to_all(a.reshape(experts, capacity, half), "ep", 0, 0, tiled=True).reshape(
        experts * capacity, half
    )
    own = exchange(pack(ids, hidden_state, experts, capacity))
    gate_part, up_part, gate_rest, up_rest, down_send, down_keep = own_part(tp, own, gate_matrix, up_matrix, down_matrix)
    act, send = hidden_part(swap(own), gate_part, up_part, gate_rest, up_rest, down_send)
    got = swap(send)
    kept = keep_part(act, down_keep)
    answers = (kept.astype(f32) + got.astype(f32)).astype(bf16)
    combined, squares = combine(ids, weights, exchange(answers), experts, capacity)
    return norm(combined, squares, swap(squares), norm_gain, half * lax.axis_size("tp"))


def solution(mesh):
    placed = (
        P(("grp", "ep"), "tp"),
        P(("grp", "ep"), None),
        P(("grp", "ep"), None),
        P("ep", None, "tp"),
        P("ep", None, "tp"),
        P("ep", "tp", None),
        P("tp"),
    )
    return jax.shard_map(
        shards, mesh=mesh, in_specs=placed, out_specs=P(("grp", "ep"), "tp"), check_vma=False
    )
```

```python
import functools

import jax
import jax.numpy as jnp
from jax import lax
from jax.experimental import pallas as pl
from jax.experimental.pallas import tpu as pltpu
from jax.sharding import PartitionSpec as P

norm_eps = 1e-05
f32, bf16, i32 = jnp.float32, jnp.bfloat16, jnp.int32
VMEM = pl.BlockSpec(memory_space=pltpu.VMEM)
SMEM = pl.BlockSpec(memory_space=pltpu.SMEM)
HBM = pl.BlockSpec(memory_space=pltpu.HBM)

COVER = pl.CostEstimate(flops=1 << 34, bytes_accessed=1 << 16, transcendentals=0)


def call(body, name, mib, in_specs, out_shape, scratch=(), cost=None):
    return pl.pallas_call(
        body,
        in_specs=in_specs,
        out_specs=jax.tree.map(lambda _: VMEM, out_shape),
        out_shape=out_shape,
        scratch_shapes=scratch,
        cost_estimate=cost,
        compiler_params=pltpu.CompilerParams(vmem_limit_bytes=mib << 20),
        name=name,
    )


def dot(a, b, dims=((1,), (0,))):
    return lax.dot_general(a, b, (dims, ((), ())), preferred_element_type=f32)


def in_hbm(array):
    return pltpu.with_memory_space_constraint(array, pltpu.HBM)


def iota(shape, dim):
    return lax.broadcasted_iota(i32, shape, dim)


def slot_ranks(ids, expert_count):
    top, rows = ids.shape
    experts = iota((expert_count, rows), 0)
    named = ids[0:1] == experts
    for k in range(1, top):
        named = named | (ids[k : k + 1] == experts)
    named = jnp.where(named, 1.0, 0.0)
    earlier = jnp.where(iota((rows, rows), 0) < iota((rows, rows), 1), 1.0, 0.0)
    return named, dot(named.astype(bf16), earlier.astype(bf16))


def pack_body(ids_hbm, hidden_hbm, out_ref, ids_ref, hidden_ref, sems, *, expert_count, capacity):
    ids_copy = pltpu.make_async_copy(ids_hbm, ids_ref, sems.at[0])
    hidden_copy = pltpu.make_async_copy(hidden_hbm, hidden_ref, sems.at[1])
    ids_copy.start()
    hidden_copy.start()
    slots = expert_count * capacity
    spread = iota((slots, expert_count), 0) // capacity == iota((slots, expert_count), 1)
    spread = jnp.where(spread, 1.0, 0.0).astype(bf16)
    ids_copy.wait()
    named, rank = slot_ranks(ids_ref[...], expert_count)
    code = jnp.where(named > 0, rank, -1.0).astype(bf16)
    wanted = dot(spread, code)
    own = (iota(wanted.shape, 0) % capacity).astype(f32)
    placing = jnp.where(wanted == own, 1.0, 0.0).astype(bf16)
    hidden_copy.wait()
    out_ref[...] = dot(placing, hidden_ref[...]).astype(bf16)


def pack(ids, hidden, expert_count, capacity):
    body = functools.partial(pack_body, expert_count=expert_count, capacity=capacity)
    out = jax.ShapeDtypeStruct((expert_count * capacity, hidden.shape[1]), bf16)
    scratch = [pltpu.VMEM(ids.shape, i32), pltpu.VMEM(hidden.shape, bf16), pltpu.SemaphoreType.DMA((2,))]
    return call(body, "pack", 4, [HBM] * 2, out, scratch, COVER)(in_hbm(ids), in_hbm(hidden))


def own_body(tp_ref, own_ref, gate_ref, up_hbm, gate_out, up_out, up_rest, up_ref, sems, *, tile):
    half = own_ref.shape[1]
    units = gate_out.shape[1]
    mine = pl.ds(pl.multiple_of(tp_ref[0] * half, half), half)
    theirs = pl.ds(pl.multiple_of((1 - tp_ref[0]) * half, half), half)
    here = pltpu.make_async_copy(up_hbm.at[0, mine, :], up_ref, sems.at[0])
    rest = pltpu.make_async_copy(up_hbm.at[0, theirs, :], up_rest, sems.at[1])
    here.start()
    rest.start()
    own = own_ref[...]
    tiles = [slice(start, start + tile) for start in range(0, units, tile)]
    for at in tiles:
        gate_out[:, at] = dot(own, gate_ref[0, mine, at])
    here.wait()
    for at in tiles:
        up_out[:, at] = dot(own, up_ref[:, at])
    rest.wait()


def own_part(tp, own, gate, up, tile=256):
    rows, half = own.shape
    units = gate.shape[2]
    cost = pl.CostEstimate(flops=4 * rows * units * half, bytes_accessed=4 * units * half, transcendentals=0)
    out = [jax.ShapeDtypeStruct((rows, units), f32)] * 2 + [jax.ShapeDtypeStruct((half, units), bf16)]
    scratch = [pltpu.VMEM((half, units), bf16), pltpu.SemaphoreType.DMA((2,))]
    body = functools.partial(own_body, tile=tile)
    return call(body, "own_part", 8, [SMEM, VMEM, VMEM, HBM], out, scratch, cost)(tp, own, gate, in_hbm(up))


def hidden_body(tp_ref, other_ref, gate_in, up_in, gate_ref, up_ref, down_hbm, act_ref, send_ref, down_keep, down_ref, sems, *, tile):
    half = other_ref.shape[1]
    mine = pl.ds(pl.multiple_of(tp_ref[0] * half, half), half)
    theirs = pl.ds(pl.multiple_of((1 - tp_ref[0]) * half, half), half)
    sent = pltpu.make_async_copy(down_hbm.at[0, :, theirs], down_ref, sems.at[0])
    kept = pltpu.make_async_copy(down_hbm.at[0, :, mine], down_keep, sems.at[1])
    sent.start()
    kept.start()
    other = other_ref[...]
    for start in range(0, gate_ref.shape[2], tile):
        at = slice(start, start + tile)
        gate = gate_in[:, at] + dot(other, gate_ref[0, theirs, at])
        up = up_in[:, at] + dot(other, up_ref[:, at])
        act_ref[:, at] = (gate / (1.0 + jnp.exp(-gate)) * up).astype(bf16)
    sent.wait()
    send_ref[...] = dot(act_ref[...], down_ref[...]).astype(bf16)
    kept.wait()


def hidden_part(tp, other, gate_in, up_in, gate, up_rest, down, tile=256):
    rows, half = other.shape
    units = gate.shape[2]
    cost = pl.CostEstimate(flops=6 * rows * units * half, bytes_accessed=6 * units * half, transcendentals=rows * units)
    shape = jax.ShapeDtypeStruct
    out = [shape((rows, units), bf16), shape((rows, half), bf16), shape((units, half), bf16)]
    scratch = [pltpu.VMEM((units, half), bf16), pltpu.SemaphoreType.DMA((2,))]
    body = functools.partial(hidden_body, tile=tile)
    return call(body, "hidden_part", 8, [SMEM] + [VMEM] * 5 + [HBM], out, scratch, cost)(
        tp, other, gate_in, up_in, gate, up_rest, in_hbm(down)
    )


def keep_body(act_ref, down_ref, out_ref):
    out_ref[...] = dot(act_ref[...], down_ref[...]).astype(bf16)


def keep_part(act, down_keep):
    rows, units = act.shape
    half = down_keep.shape[1]
    cost = pl.CostEstimate(flops=2 * rows * units * half, bytes_accessed=2 * units * half, transcendentals=0)
    return call(keep_body, "keep_part", 8, [VMEM] * 2, jax.ShapeDtypeStruct((rows, half), bf16), cost=cost)(act, down_keep)


def combine_body(ids_ref, weight_ref, back_ref, out_ref, square_ref, *, expert_count, capacity):
    ids = ids_ref[...]
    top, rows = ids.shape
    _, rank = slot_ranks(ids, expert_count)
    experts = iota((expert_count, rows), 0)
    places = iota((expert_count * capacity, rows), 0)
    weights = jnp.zeros(places.shape, f32)
    for k in range(top):
        row = ids[k : k + 1]
        at = jnp.sum(jnp.where(row == experts, rank, 0.0), axis=0, keepdims=True).astype(i32)
        weights += jnp.where(row * capacity + at == places, weight_ref[k : k + 1], 0.0)
    high = weights.astype(bf16)
    low = (weights - high.astype(f32)).astype(bf16)
    back = back_ref[...]
    over = ((0,), (0,))
    combined = dot(high, back, over) + dot(low, back, over)
    out_ref[...] = combined
    square_ref[...] = jnp.broadcast_to(jnp.sum(combined * combined, axis=1, keepdims=True), square_ref.shape)


def combine(ids, weights, back, expert_count, capacity):
    rows = ids.shape[1]
    body = functools.partial(combine_body, expert_count=expert_count, capacity=capacity)
    out = [jax.ShapeDtypeStruct((rows, back.shape[1]), f32), jax.ShapeDtypeStruct((rows, 128), f32)]
    return call(body, "combine", 4, [VMEM] * 3, out)(ids, weights, back)


def norm_body(combined_ref, square_ref, other_ref, gain_ref, out_ref, *, width):
    total = (square_ref[...] + other_ref[...])[:, 0:1]
    out_ref[...] = (combined_ref[...] * lax.rsqrt(total / width + norm_eps) * gain_ref[...]).astype(bf16)


def norm(combined, squares, others, gain, width):
    body = functools.partial(norm_body, width=width)
    out = jax.ShapeDtypeStruct(combined.shape, bf16)
    return call(body, "norm", 4, [VMEM] * 4, out)(combined, squares, others, gain.reshape(1, -1))


def shards(hidden_state, expert_ids, route_weight, gate_matrix, up_matrix, down_matrix, norm_gain):
    tok_count, top_count = expert_ids.shape
    half = hidden_state.shape[1]
    experts = lax.axis_size("ep")
    capacity = max(2, 2 * tok_count * top_count // experts)
    tp = lax.axis_index("tp").reshape(1)
    ids, weights = expert_ids.T, route_weight.T
    swap = lambda a: lax.ppermute(a, "tp", [(0, 1), (1, 0)])
    exchange = lambda a: lax.all_to_all(a.reshape(experts, capacity, half), "ep", 0, 0, tiled=True).reshape(
        experts * capacity, half
    )
    own = exchange(pack(ids, hidden_state, experts, capacity))
    gate_part, up_part, up_rest = own_part(tp, own, gate_matrix, up_matrix)
    act, send, down_keep = hidden_part(tp, swap(own), gate_part, up_part, gate_matrix, up_rest, down_matrix)
    got = swap(send)
    kept = keep_part(act, down_keep)
    answers = (kept.astype(f32) + got.astype(f32)).astype(bf16)
    combined, squares = combine(ids, weights, exchange(answers), experts, capacity)
    return norm(combined, squares, swap(squares), norm_gain, half * lax.axis_size("tp"))


def solution(mesh):
    placed = (
        P(("grp", "ep"), "tp"),
        P(("grp", "ep"), None),
        P(("grp", "ep"), None),
        P("ep", None, "tp"),
        P("ep", None, "tp"),
        P("ep", "tp", None),
        P("tp"),
    )
    return jax.shard_map(
        shards, mesh=mesh, in_specs=placed, out_specs=P(("grp", "ep"), "tp"), check_vma=False
    )
```

```python
import functools

import jax
import jax.numpy as jnp
from jax import lax
from jax.experimental import pallas as pl
from jax.experimental.pallas import tpu as pltpu
from jax.sharding import PartitionSpec as P

norm_eps = 1e-05
f32, bf16, i32 = jnp.float32, jnp.bfloat16, jnp.int32
VMEM = pl.BlockSpec(memory_space=pltpu.VMEM)
SMEM = pl.BlockSpec(memory_space=pltpu.SMEM)
HBM = pl.BlockSpec(memory_space=pltpu.HBM)

COVER = pl.CostEstimate(flops=1 << 34, bytes_accessed=1 << 16, transcendentals=0)


def call(body, name, mib, in_specs, out_shape, scratch=(), cost=None):
    return pl.pallas_call(
        body,
        in_specs=in_specs,
        out_specs=jax.tree.map(lambda _: VMEM, out_shape),
        out_shape=out_shape,
        scratch_shapes=scratch,
        cost_estimate=cost,
        compiler_params=pltpu.CompilerParams(vmem_limit_bytes=mib << 20),
        name=name,
    )


def dot(a, b, dims=((1,), (0,))):
    return lax.dot_general(a, b, (dims, ((), ())), preferred_element_type=f32)


def in_hbm(array):
    return pltpu.with_memory_space_constraint(array, pltpu.HBM)


def iota(shape, dim):
    return lax.broadcasted_iota(i32, shape, dim)


def slot_ranks(ids, expert_count):
    top, rows = ids.shape
    experts = iota((expert_count, rows), 0)
    named = ids[0:1] == experts
    for k in range(1, top):
        named = named | (ids[k : k + 1] == experts)
    named = jnp.where(named, 1.0, 0.0)
    earlier = jnp.where(iota((rows, rows), 0) < iota((rows, rows), 1), 1.0, 0.0)
    return named, dot(named.astype(bf16), earlier.astype(bf16))


def pack_body(ids_hbm, hidden_hbm, out_ref, ids_ref, hidden_ref, sems, *, expert_count, capacity):
    ids_copy = pltpu.make_async_copy(ids_hbm, ids_ref, sems.at[0])
    hidden_copy = pltpu.make_async_copy(hidden_hbm, hidden_ref, sems.at[1])
    ids_copy.start()
    hidden_copy.start()
    slots = expert_count * capacity
    spread = iota((slots, expert_count), 0) // capacity == iota((slots, expert_count), 1)
    spread = jnp.where(spread, 1.0, 0.0).astype(bf16)
    ids_copy.wait()
    named, rank = slot_ranks(ids_ref[...], expert_count)
    code = jnp.where(named > 0, rank, -1.0).astype(bf16)
    wanted = dot(spread, code)
    own = (iota(wanted.shape, 0) % capacity).astype(f32)
    placing = jnp.where(wanted == own, 1.0, 0.0).astype(bf16)
    hidden_copy.wait()
    out_ref[...] = dot(placing, hidden_ref[...]).astype(bf16)


def pack(ids, hidden, expert_count, capacity):
    body = functools.partial(pack_body, expert_count=expert_count, capacity=capacity)
    out = jax.ShapeDtypeStruct((expert_count * capacity, hidden.shape[1]), bf16)
    scratch = [pltpu.VMEM(ids.shape, i32), pltpu.VMEM(hidden.shape, bf16), pltpu.SemaphoreType.DMA((2,))]
    return call(body, "pack", 4, [HBM] * 2, out, scratch, COVER)(in_hbm(ids), in_hbm(hidden))


def own_body(tp_ref, own_ref, gate_ref, up_hbm, down_hbm, gate_out, up_out, up_rest, down_send, up_ref, sems, *, tile):
    half = own_ref.shape[1]
    units = gate_out.shape[1]
    mine = pl.ds(pl.multiple_of(tp_ref[0] * half, half), half)
    theirs = pl.ds(pl.multiple_of((1 - tp_ref[0]) * half, half), half)
    here = pltpu.make_async_copy(up_hbm.at[0, mine, :], up_ref, sems.at[0])
    rest = pltpu.make_async_copy(up_hbm.at[0, theirs, :], up_rest, sems.at[1])
    down = pltpu.make_async_copy(down_hbm.at[0, :, theirs], down_send, sems.at[2])
    here.start()
    own = own_ref[...]
    for start in range(0, units, tile):
        if start == tile:
            rest.start()
            down.start()
        at = slice(start, start + tile)
        gate_out[:, at] = dot(own, gate_ref[0, mine, at])
    here.wait()
    for start in range(0, units, tile):
        at = slice(start, start + tile)
        up_out[:, at] = dot(own, up_ref[:, at])
    rest.wait()
    down.wait()


def own_part(tp, own, gate, up, down, tile=256):
    rows, half = own.shape
    units = gate.shape[2]
    cost = pl.CostEstimate(flops=4 * rows * units * half, bytes_accessed=4 * units * half, transcendentals=0)
    shape = jax.ShapeDtypeStruct
    out = [shape((rows, units), f32)] * 2 + [shape((half, units), bf16), shape((units, half), bf16)]
    scratch = [pltpu.VMEM((half, units), bf16), pltpu.SemaphoreType.DMA((3,))]
    body = functools.partial(own_body, tile=tile)
    specs = [SMEM, VMEM, VMEM, HBM, HBM]
    return call(body, "own_part", 8, specs, out, scratch, cost)(tp, own, gate, in_hbm(up), in_hbm(down))


def hidden_body(tp_ref, other_ref, gate_in, up_in, gate_ref, up_ref, down_ref, down_hbm, act_ref, send_ref, down_keep, sems, *, tile):
    half = other_ref.shape[1]
    mine = pl.ds(pl.multiple_of(tp_ref[0] * half, half), half)
    theirs = pl.ds(pl.multiple_of((1 - tp_ref[0]) * half, half), half)
    kept = pltpu.make_async_copy(down_hbm.at[0, :, mine], down_keep, sems.at[0])
    kept.start()
    other = other_ref[...]
    for start in range(0, gate_ref.shape[2], tile):
        at = slice(start, start + tile)
        gate = gate_in[:, at] + dot(other, gate_ref[0, theirs, at])
        up = up_in[:, at] + dot(other, up_ref[:, at])
        act_ref[:, at] = (gate / (1.0 + jnp.exp(-gate)) * up).astype(bf16)
    send_ref[...] = dot(act_ref[...], down_ref[...]).astype(bf16)
    kept.wait()


def hidden_part(tp, other, gate_in, up_in, gate, up_rest, down_send, down, tile=256):
    rows, half = other.shape
    units = gate.shape[2]
    cost = pl.CostEstimate(flops=6 * rows * units * half, bytes_accessed=6 * units * half, transcendentals=rows * units)
    shape = jax.ShapeDtypeStruct
    out = [shape((rows, units), bf16), shape((rows, half), bf16), shape((units, half), bf16)]
    body = functools.partial(hidden_body, tile=tile)
    return call(body, "hidden_part", 8, [SMEM] + [VMEM] * 6 + [HBM], out, [pltpu.SemaphoreType.DMA((1,))], cost)(
        tp, other, gate_in, up_in, gate, up_rest, down_send, in_hbm(down)
    )


def keep_body(act_ref, down_ref, out_ref):
    out_ref[...] = dot(act_ref[...], down_ref[...]).astype(bf16)


def keep_part(act, down_keep):
    rows, units = act.shape
    half = down_keep.shape[1]
    cost = pl.CostEstimate(flops=2 * rows * units * half, bytes_accessed=2 * units * half, transcendentals=0)
    return call(keep_body, "keep_part", 8, [VMEM] * 2, jax.ShapeDtypeStruct((rows, half), bf16), cost=cost)(act, down_keep)


def weigh_body(ids_ref, weight_ref, high_ref, low_ref, *, expert_count, capacity):
    ids = ids_ref[...]
    top, rows = ids.shape
    _, rank = slot_ranks(ids, expert_count)
    experts = iota((expert_count, rows), 0)
    places = iota((expert_count * capacity, rows), 0)
    weights = jnp.zeros(places.shape, f32)
    for k in range(top):
        row = ids[k : k + 1]
        at = jnp.sum(jnp.where(row == experts, rank, 0.0), axis=0, keepdims=True).astype(i32)
        weights += jnp.where(row * capacity + at == places, weight_ref[k : k + 1], 0.0)
    high = weights.astype(bf16)
    high_ref[...] = high
    low_ref[...] = (weights - high.astype(f32)).astype(bf16)


def weigh(ids, weights, expert_count, capacity):
    body = functools.partial(weigh_body, expert_count=expert_count, capacity=capacity)
    out = [jax.ShapeDtypeStruct((expert_count * capacity, ids.shape[1]), bf16)] * 2
    return call(body, "weigh", 4, [VMEM] * 2, out)(ids, weights)


def combine_body(high_ref, low_ref, back_ref, out_ref, square_ref):
    back = back_ref[...]
    over = ((0,), (0,))
    combined = dot(high_ref[...], back, over) + dot(low_ref[...], back, over)
    out_ref[...] = combined
    square_ref[...] = jnp.broadcast_to(jnp.sum(combined * combined, axis=1, keepdims=True), square_ref.shape)


def combine(high, low, back):
    rows = high.shape[1]
    out = [jax.ShapeDtypeStruct((rows, back.shape[1]), f32), jax.ShapeDtypeStruct((rows, 128), f32)]
    return call(combine_body, "combine", 4, [VMEM] * 3, out)(high, low, back)


def norm_body(combined_ref, square_ref, other_ref, gain_ref, out_ref, *, width):
    total = (square_ref[...] + other_ref[...])[:, 0:1]
    out_ref[...] = (combined_ref[...] * lax.rsqrt(total / width + norm_eps) * gain_ref[...]).astype(bf16)


def norm(combined, squares, others, gain, width):
    body = functools.partial(norm_body, width=width)
    out = jax.ShapeDtypeStruct(combined.shape, bf16)
    return call(body, "norm", 4, [VMEM] * 4, out)(combined, squares, others, gain.reshape(1, -1))


def shards(hidden_state, expert_ids, route_weight, gate_matrix, up_matrix, down_matrix, norm_gain):
    tok_count, top_count = expert_ids.shape
    half = hidden_state.shape[1]
    experts = lax.axis_size("ep")
    capacity = max(2, 2 * tok_count * top_count // experts)
    tp = lax.axis_index("tp").reshape(1)
    ids, weights = expert_ids.T, route_weight.T
    swap = lambda a: lax.ppermute(a, "tp", [(0, 1), (1, 0)])
    exchange = lambda a: lax.all_to_all(a.reshape(experts, capacity, half), "ep", 0, 0, tiled=True).reshape(
        experts * capacity, half
    )
    own = exchange(pack(ids, hidden_state, experts, capacity))
    gate_part, up_part, up_rest, down_send = own_part(tp, own, gate_matrix, up_matrix, down_matrix)
    act, send, down_keep = hidden_part(
        tp, swap(own), gate_part, up_part, gate_matrix, up_rest, down_send, down_matrix
    )
    got = swap(send)
    kept = keep_part(act, down_keep)
    kept, high, low = lax.optimization_barrier((kept, *weigh(ids, weights, experts, capacity)))
    answers = (kept.astype(f32) + got.astype(f32)).astype(bf16)
    combined, squares = combine(high, low, exchange(answers))
    return norm(combined, squares, swap(squares), norm_gain, half * lax.axis_size("tp"))


def solution(mesh):
    placed = (
        P(("grp", "ep"), "tp"),
        P(("grp", "ep"), None),
        P(("grp", "ep"), None),
        P("ep", None, "tp"),
        P("ep", None, "tp"),
        P("ep", "tp", None),
        P("tp"),
    )
    return jax.shard_map(
        shards, mesh=mesh, in_specs=placed, out_specs=P(("grp", "ep"), "tp"), check_vma=False
    )
```

```python
import functools

import jax
import jax.numpy as jnp
from jax import lax
from jax.experimental import pallas as pl
from jax.experimental.pallas import tpu as pltpu
from jax.sharding import PartitionSpec as P

norm_eps = 1e-05
f32, bf16, i32 = jnp.float32, jnp.bfloat16, jnp.int32
VMEM = pl.BlockSpec(memory_space=pltpu.VMEM)
SMEM = pl.BlockSpec(memory_space=pltpu.SMEM)
HBM = pl.BlockSpec(memory_space=pltpu.HBM)

COVER = pl.CostEstimate(flops=1 << 34, bytes_accessed=1 << 16, transcendentals=0)


def call(body, name, mib, in_specs, out_shape, scratch=(), cost=None):
    return pl.pallas_call(
        body,
        in_specs=in_specs,
        out_specs=jax.tree.map(lambda _: VMEM, out_shape),
        out_shape=out_shape,
        scratch_shapes=scratch,
        cost_estimate=cost,
        compiler_params=pltpu.CompilerParams(vmem_limit_bytes=mib << 20),
        name=name,
    )


def dot(a, b, dims=((1,), (0,))):
    return lax.dot_general(a, b, (dims, ((), ())), preferred_element_type=f32)


def in_hbm(array):
    return pltpu.with_memory_space_constraint(array, pltpu.HBM)


def iota(shape, dim):
    return lax.broadcasted_iota(i32, shape, dim)


def slot_ranks(ids, expert_count):
    top, rows = ids.shape
    experts = iota((expert_count, rows), 0)
    named = ids[0:1] == experts
    for k in range(1, top):
        named = named | (ids[k : k + 1] == experts)
    named = jnp.where(named, 1.0, 0.0)
    earlier = jnp.where(iota((rows, rows), 0) < iota((rows, rows), 1), 1.0, 0.0)
    return named, dot(named.astype(bf16), earlier.astype(bf16))


def pack_body(ids_hbm, hidden_hbm, out_ref, ids_ref, hidden_ref, sems, *, expert_count, capacity):
    ids_copy = pltpu.make_async_copy(ids_hbm, ids_ref, sems.at[0])
    hidden_copy = pltpu.make_async_copy(hidden_hbm, hidden_ref, sems.at[1])
    ids_copy.start()
    hidden_copy.start()
    slots = expert_count * capacity
    spread = iota((slots, expert_count), 0) // capacity == iota((slots, expert_count), 1)
    spread = jnp.where(spread, 1.0, 0.0).astype(bf16)
    ids_copy.wait()
    named, rank = slot_ranks(ids_ref[...], expert_count)
    code = jnp.where(named > 0, rank, -1.0).astype(bf16)
    wanted = dot(spread, code)
    own = (iota(wanted.shape, 0) % capacity).astype(f32)
    placing = jnp.where(wanted == own, 1.0, 0.0).astype(bf16)
    hidden_copy.wait()
    out_ref[...] = dot(placing, hidden_ref[...]).astype(bf16)


def pack(ids, hidden, expert_count, capacity):
    body = functools.partial(pack_body, expert_count=expert_count, capacity=capacity)
    out = jax.ShapeDtypeStruct((expert_count * capacity, hidden.shape[1]), bf16)
    scratch = [pltpu.VMEM(ids.shape, i32), pltpu.VMEM(hidden.shape, bf16), pltpu.SemaphoreType.DMA((2,))]
    return call(body, "pack", 4, [HBM] * 2, out, scratch, COVER)(in_hbm(ids), in_hbm(hidden))


def own_body(tp_ref, own_ref, gate_ref, up_hbm, down_hbm, gate_out, up_out, up_rest, down_send, up_ref, sems, *, tile):
    half = own_ref.shape[1]
    units = gate_out.shape[1]
    mine = pl.ds(pl.multiple_of(tp_ref[0] * half, half), half)
    theirs = pl.ds(pl.multiple_of((1 - tp_ref[0]) * half, half), half)
    here = pltpu.make_async_copy(up_hbm.at[0, mine, :], up_ref, sems.at[0])
    rest = pltpu.make_async_copy(up_hbm.at[0, theirs, :], up_rest, sems.at[1])
    down = pltpu.make_async_copy(down_hbm.at[0, :, theirs], down_send, sems.at[2])
    here.start()
    own = own_ref[...]
    for start in range(0, units, tile):
        if start == tile:
            rest.start()
            down.start()
        at = slice(start, start + tile)
        gate_out[:, at] = dot(own, gate_ref[0, mine, at])
    here.wait()
    for start in range(0, units, tile):
        at = slice(start, start + tile)
        up_out[:, at] = dot(own, up_ref[:, at])
    rest.wait()
    down.wait()


def own_part(tp, own, gate, up, down, tile=256):
    rows, half = own.shape
    units = gate.shape[2]
    cost = pl.CostEstimate(flops=4 * rows * units * half, bytes_accessed=4 * units * half, transcendentals=0)
    shape = jax.ShapeDtypeStruct
    out = [shape((rows, units), f32)] * 2 + [shape((half, units), bf16), shape((units, half), bf16)]
    scratch = [pltpu.VMEM((half, units), bf16), pltpu.SemaphoreType.DMA((3,))]
    body = functools.partial(own_body, tile=tile)
    specs = [SMEM, VMEM, VMEM, HBM, HBM]
    return call(body, "own_part", 8, specs, out, scratch, cost)(tp, own, gate, in_hbm(up), in_hbm(down))


def hidden_body(tp_ref, other_ref, gate_in, up_in, gate_ref, up_ref, down_ref, act_ref, send_ref, *, tile):
    half = other_ref.shape[1]
    theirs = pl.ds(pl.multiple_of((1 - tp_ref[0]) * half, half), half)
    other = other_ref[...]
    for start in range(0, gate_ref.shape[2], tile):
        at = slice(start, start + tile)
        gate = gate_in[:, at] + dot(other, gate_ref[0, theirs, at])
        up = up_in[:, at] + dot(other, up_ref[:, at])
        act_ref[:, at] = (gate / (1.0 + jnp.exp(-gate)) * up).astype(bf16)
    send_ref[...] = dot(act_ref[...], down_ref[...]).astype(bf16)


def hidden_part(tp, other, gate_in, up_in, gate, up_rest, down_send, tile=256):
    rows, half = other.shape
    units = gate.shape[2]
    cost = pl.CostEstimate(flops=6 * rows * units * half, bytes_accessed=6 * units * half, transcendentals=rows * units)
    out = [jax.ShapeDtypeStruct((rows, units), bf16), jax.ShapeDtypeStruct((rows, half), bf16)]
    body = functools.partial(hidden_body, tile=tile)
    return call(body, "hidden_part", 8, [SMEM] + [VMEM] * 6, out, cost=cost)(
        tp, other, gate_in, up_in, gate, up_rest, down_send
    )


def keep_body(tp_ref, act_ref, down_ref, out_ref):
    half = out_ref.shape[1]
    mine = pl.ds(pl.multiple_of(tp_ref[0] * half, half), half)
    out_ref[...] = dot(act_ref[...], down_ref[0, :, mine]).astype(bf16)


def keep_part(tp, act, down, half):
    rows, units = act.shape
    cost = pl.CostEstimate(flops=2 * rows * units * half, bytes_accessed=2 * units * half, transcendentals=0)
    out = jax.ShapeDtypeStruct((rows, half), bf16)
    return call(keep_body, "keep_part", 8, [SMEM] + [VMEM] * 2, out, cost=cost)(tp, act, down)


def weigh_body(ids_ref, weight_ref, high_ref, low_ref, *, expert_count, capacity):
    ids = ids_ref[...]
    top, rows = ids.shape
    _, rank = slot_ranks(ids, expert_count)
    experts = iota((expert_count, rows), 0)
    places = iota((expert_count * capacity, rows), 0)
    weights = jnp.zeros(places.shape, f32)
    for k in range(top):
        row = ids[k : k + 1]
        at = jnp.sum(jnp.where(row == experts, rank, 0.0), axis=0, keepdims=True).astype(i32)
        weights += jnp.where(row * capacity + at == places, weight_ref[k : k + 1], 0.0)
    high = weights.astype(bf16)
    high_ref[...] = high
    low_ref[...] = (weights - high.astype(f32)).astype(bf16)


def weigh(ids, weights, expert_count, capacity):
    body = functools.partial(weigh_body, expert_count=expert_count, capacity=capacity)
    out = [jax.ShapeDtypeStruct((expert_count * capacity, ids.shape[1]), bf16)] * 2
    return call(body, "weigh", 4, [VMEM] * 2, out)(ids, weights)


def combine_body(high_ref, low_ref, back_ref, out_ref, square_ref):
    back = back_ref[...]
    over = ((0,), (0,))
    combined = dot(high_ref[...], back, over) + dot(low_ref[...], back, over)
    out_ref[...] = combined
    square_ref[...] = jnp.broadcast_to(jnp.sum(combined * combined, axis=1, keepdims=True), square_ref.shape)


def combine(high, low, back):
    rows = high.shape[1]
    out = [jax.ShapeDtypeStruct((rows, back.shape[1]), f32), jax.ShapeDtypeStruct((rows, 128), f32)]
    return call(combine_body, "combine", 4, [VMEM] * 3, out)(high, low, back)


def norm_body(combined_ref, square_ref, other_ref, gain_ref, out_ref, *, width):
    total = (square_ref[...] + other_ref[...])[:, 0:1]
    out_ref[...] = (combined_ref[...] * lax.rsqrt(total / width + norm_eps) * gain_ref[...]).astype(bf16)


def norm(combined, squares, others, gain, width):
    body = functools.partial(norm_body, width=width)
    out = jax.ShapeDtypeStruct(combined.shape, bf16)
    return call(body, "norm", 4, [VMEM] * 4, out)(combined, squares, others, gain.reshape(1, -1))


def shards(hidden_state, expert_ids, route_weight, gate_matrix, up_matrix, down_matrix, norm_gain):
    tok_count, top_count = expert_ids.shape
    half = hidden_state.shape[1]
    experts = lax.axis_size("ep")
    capacity = max(2, 2 * tok_count * top_count // experts)
    tp = lax.axis_index("tp").reshape(1)
    ids, weights = expert_ids.T, route_weight.T
    swap = lambda a: lax.ppermute(a, "tp", [(0, 1), (1, 0)])
    exchange = lambda a: lax.all_to_all(a.reshape(experts, capacity, half), "ep", 0, 0, tiled=True).reshape(
        experts * capacity, half
    )
    own = exchange(pack(ids, hidden_state, experts, capacity))
    gate_part, up_part, up_rest, down_send = own_part(tp, own, gate_matrix, up_matrix, down_matrix)
    act, send = hidden_part(tp, swap(own), gate_part, up_part, gate_matrix, up_rest, down_send)
    got = swap(send)
    kept = keep_part(tp, act, down_matrix, half)
    kept, high, low = lax.optimization_barrier((kept, *weigh(ids, weights, experts, capacity)))
    answers = (kept.astype(f32) + got.astype(f32)).astype(bf16)
    combined, squares = combine(high, low, exchange(answers))
    return norm(combined, squares, swap(squares), norm_gain, half * lax.axis_size("tp"))


def solution(mesh):
    placed = (
        P(("grp", "ep"), "tp"),
        P(("grp", "ep"), None),
        P(("grp", "ep"), None),
        P("ep", None, "tp"),
        P("ep", None, "tp"),
        P("ep", "tp", None),
        P("tp"),
    )
    return jax.shard_map(
        shards, mesh=mesh, in_specs=placed, out_specs=P(("grp", "ep"), "tp"), check_vma=False
    )
```

```python
import functools

import jax
import jax.numpy as jnp
from jax import lax
from jax.experimental import pallas as pl
from jax.experimental.pallas import tpu as pltpu
from jax.sharding import PartitionSpec as P

norm_eps = 1e-05
f32, bf16, i32 = jnp.float32, jnp.bfloat16, jnp.int32
VMEM = pl.BlockSpec(memory_space=pltpu.VMEM)
SMEM = pl.BlockSpec(memory_space=pltpu.SMEM)
HBM = pl.BlockSpec(memory_space=pltpu.HBM)

COVER = pl.CostEstimate(flops=1 << 34, bytes_accessed=1 << 16, transcendentals=0)


def call(body, name, mib, in_specs, out_shape, scratch=(), cost=None):
    return pl.pallas_call(
        body,
        in_specs=in_specs,
        out_specs=jax.tree.map(lambda _: VMEM, out_shape),
        out_shape=out_shape,
        scratch_shapes=scratch,
        cost_estimate=cost,
        compiler_params=pltpu.CompilerParams(vmem_limit_bytes=mib << 20),
        name=name,
    )


def dot(a, b, dims=((1,), (0,))):
    return lax.dot_general(a, b, (dims, ((), ())), preferred_element_type=f32)


def in_hbm(array):
    return pltpu.with_memory_space_constraint(array, pltpu.HBM)


def iota(shape, dim):
    return lax.broadcasted_iota(i32, shape, dim)


def slot_ranks(ids, expert_count):
    top, rows = ids.shape
    experts = iota((expert_count, rows), 0)
    named = ids[0:1] == experts
    for k in range(1, top):
        named = named | (ids[k : k + 1] == experts)
    named = jnp.where(named, 1.0, 0.0)
    earlier = jnp.where(iota((rows, rows), 0) < iota((rows, rows), 1), 1.0, 0.0)
    return named, dot(named.astype(bf16), earlier.astype(bf16))


def pack_body(ids_hbm, hidden_hbm, out_ref, ids_ref, hidden_ref, sems, *, expert_count, capacity):
    ids_copy = pltpu.make_async_copy(ids_hbm, ids_ref, sems.at[0])
    hidden_copy = pltpu.make_async_copy(hidden_hbm, hidden_ref, sems.at[1])
    ids_copy.start()
    hidden_copy.start()
    slots = expert_count * capacity
    spread = iota((slots, expert_count), 0) // capacity == iota((slots, expert_count), 1)
    spread = jnp.where(spread, 1.0, 0.0).astype(bf16)
    ids_copy.wait()
    named, rank = slot_ranks(ids_ref[...], expert_count)
    code = jnp.where(named > 0, rank, -1.0).astype(bf16)
    wanted = dot(spread, code)
    own = (iota(wanted.shape, 0) % capacity).astype(f32)
    placing = jnp.where(wanted == own, 1.0, 0.0).astype(bf16)
    hidden_copy.wait()
    out_ref[...] = dot(placing, hidden_ref[...]).astype(bf16)


def pack(ids, hidden, expert_count, capacity):
    body = functools.partial(pack_body, expert_count=expert_count, capacity=capacity)
    out = jax.ShapeDtypeStruct((expert_count * capacity, hidden.shape[1]), bf16)
    scratch = [pltpu.VMEM(ids.shape, i32), pltpu.VMEM(hidden.shape, bf16), pltpu.SemaphoreType.DMA((2,))]
    return call(body, "pack", 4, [HBM] * 2, out, scratch, COVER)(in_hbm(ids), in_hbm(hidden))


def own_body(tp_ref, own_ref, gate_ref, up_hbm, gate_out, up_out, up_rest, up_ref, sems, *, tile):
    half = own_ref.shape[1]
    units = gate_out.shape[1]
    mine = pl.ds(pl.multiple_of(tp_ref[0] * half, half), half)
    theirs = pl.ds(pl.multiple_of((1 - tp_ref[0]) * half, half), half)
    here = pltpu.make_async_copy(up_hbm.at[0, mine, :], up_ref, sems.at[0])
    rest = pltpu.make_async_copy(up_hbm.at[0, theirs, :], up_rest, sems.at[1])
    here.start()
    rest.start()
    own = own_ref[...]
    for start in range(0, units, tile):
        at = slice(start, start + tile)
        gate_out[:, at] = dot(own, gate_ref[0, mine, at])
    here.wait()
    for start in range(0, units, tile):
        at = slice(start, start + tile)
        up_out[:, at] = dot(own, up_ref[:, at])
    rest.wait()


def own_part(tp, own, gate, up, tile=256):
    rows, half = own.shape
    units = gate.shape[2]
    shape = jax.ShapeDtypeStruct
    out = [shape((rows, units), f32)] * 2 + [shape((half, units), bf16)]
    scratch = [pltpu.VMEM((half, units), bf16), pltpu.SemaphoreType.DMA((2,))]
    body = functools.partial(own_body, tile=tile)
    return call(body, "own_part", 8, [SMEM, VMEM, VMEM, HBM], out, scratch)(tp, own, gate, in_hbm(up))


def hidden_body(tp_ref, other_ref, gate_in, up_in, gate_ref, up_ref, down_ref, act_ref, send_ref, *, tile):
    half = other_ref.shape[1]
    theirs = pl.ds(pl.multiple_of((1 - tp_ref[0]) * half, half), half)
    other = other_ref[...]
    for start in range(0, gate_ref.shape[2], tile):
        at = slice(start, start + tile)
        gate = gate_in[:, at] + dot(other, gate_ref[0, theirs, at])
        up = up_in[:, at] + dot(other, up_ref[:, at])
        act_ref[:, at] = (gate / (1.0 + jnp.exp(-gate)) * up).astype(bf16)
    send_ref[...] = dot(act_ref[...], down_ref[0, :, theirs]).astype(bf16)


def hidden_part(tp, other, gate_in, up_in, gate, up_rest, down, tile=256):
    rows, half = other.shape
    units = gate.shape[2]
    cost = pl.CostEstimate(flops=6 * rows * units * half, bytes_accessed=6 * units * half, transcendentals=rows * units)
    out = [jax.ShapeDtypeStruct((rows, units), bf16), jax.ShapeDtypeStruct((rows, half), bf16)]
    body = functools.partial(hidden_body, tile=tile)
    return call(body, "hidden_part", 8, [SMEM] + [VMEM] * 6, out, cost=cost)(
        tp, other, gate_in, up_in, gate, up_rest, down
    )


def keep_body(tp_ref, act_ref, down_ref, out_ref):
    half = out_ref.shape[1]
    mine = pl.ds(pl.multiple_of(tp_ref[0] * half, half), half)
    out_ref[...] = dot(act_ref[...], down_ref[0, :, mine]).astype(bf16)


def keep_part(tp, act, down, half):
    rows, units = act.shape
    cost = pl.CostEstimate(flops=2 * rows * units * half, bytes_accessed=2 * units * half, transcendentals=0)
    out = jax.ShapeDtypeStruct((rows, half), bf16)
    return call(keep_body, "keep_part", 8, [SMEM] + [VMEM] * 2, out, cost=cost)(tp, act, down)


def weigh_body(ids_ref, weight_ref, high_ref, low_ref, *, expert_count, capacity):
    ids = ids_ref[...]
    top, rows = ids.shape
    _, rank = slot_ranks(ids, expert_count)
    experts = iota((expert_count, rows), 0)
    places = iota((expert_count * capacity, rows), 0)
    weights = jnp.zeros(places.shape, f32)
    for k in range(top):
        row = ids[k : k + 1]
        at = jnp.sum(jnp.where(row == experts, rank, 0.0), axis=0, keepdims=True).astype(i32)
        weights += jnp.where(row * capacity + at == places, weight_ref[k : k + 1], 0.0)
    high = weights.astype(bf16)
    high_ref[...] = high
    low_ref[...] = (weights - high.astype(f32)).astype(bf16)


def weigh(ids, weights, expert_count, capacity):
    body = functools.partial(weigh_body, expert_count=expert_count, capacity=capacity)
    out = [jax.ShapeDtypeStruct((expert_count * capacity, ids.shape[1]), bf16)] * 2
    return call(body, "weigh", 4, [VMEM] * 2, out)(ids, weights)


def combine_body(high_ref, low_ref, back_ref, out_ref, square_ref):
    back = back_ref[...]
    over = ((0,), (0,))
    combined = dot(high_ref[...], back, over) + dot(low_ref[...], back, over)
    out_ref[...] = combined
    square_ref[...] = jnp.broadcast_to(jnp.sum(combined * combined, axis=1, keepdims=True), square_ref.shape)


def combine(high, low, back):
    rows = high.shape[1]
    out = [jax.ShapeDtypeStruct((rows, back.shape[1]), f32), jax.ShapeDtypeStruct((rows, 128), f32)]
    return call(combine_body, "combine", 4, [VMEM] * 3, out)(high, low, back)


def norm_body(combined_ref, square_ref, other_ref, gain_ref, out_ref, *, width):
    total = (square_ref[...] + other_ref[...])[:, 0:1]
    out_ref[...] = (combined_ref[...] * lax.rsqrt(total / width + norm_eps) * gain_ref[...]).astype(bf16)


def norm(combined, squares, others, gain, width):
    body = functools.partial(norm_body, width=width)
    out = jax.ShapeDtypeStruct(combined.shape, bf16)
    return call(body, "norm", 4, [VMEM] * 4, out)(combined, squares, others, gain.reshape(1, -1))


def shards(hidden_state, expert_ids, route_weight, gate_matrix, up_matrix, down_matrix, norm_gain):
    tok_count, top_count = expert_ids.shape
    half = hidden_state.shape[1]
    experts = lax.axis_size("ep")
    capacity = max(2, 2 * tok_count * top_count // experts)
    tp = lax.axis_index("tp").reshape(1)
    ids, weights = expert_ids.T, route_weight.T
    swap = lambda a: lax.ppermute(a, "tp", [(0, 1), (1, 0)])
    exchange = lambda a: lax.all_to_all(a.reshape(experts, capacity, half), "ep", 0, 0, tiled=True).reshape(
        experts * capacity, half
    )
    own = exchange(pack(ids, hidden_state, experts, capacity))
    gate_part, up_part, up_rest = own_part(tp, own, gate_matrix, up_matrix)
    act, send = hidden_part(tp, swap(own), gate_part, up_part, gate_matrix, up_rest, down_matrix)
    got = swap(send)
    kept = keep_part(tp, act, down_matrix, half)
    kept, high, low = lax.optimization_barrier((kept, *weigh(ids, weights, experts, capacity)))
    answers = (kept.astype(f32) + got.astype(f32)).astype(bf16)
    combined, squares = combine(high, low, exchange(answers))
    return norm(combined, squares, swap(squares), norm_gain, half * lax.axis_size("tp"))


def solution(mesh):
    placed = (
        P(("grp", "ep"), "tp"),
        P(("grp", "ep"), None),
        P(("grp", "ep"), None),
        P("ep", None, "tp"),
        P("ep", None, "tp"),
        P("ep", "tp", None),
        P("tp"),
    )
    return jax.shard_map(
        shards, mesh=mesh, in_specs=placed, out_specs=P(("grp", "ep"), "tp"), check_vma=False
    )
```

```python
import functools

import jax
import jax.numpy as jnp
from jax import lax
from jax.experimental import pallas as pl
from jax.experimental.pallas import tpu as pltpu
from jax.sharding import PartitionSpec as P

norm_eps = 1e-05
f32, bf16, i32 = jnp.float32, jnp.bfloat16, jnp.int32
VMEM = pl.BlockSpec(memory_space=pltpu.VMEM)
SMEM = pl.BlockSpec(memory_space=pltpu.SMEM)
HBM = pl.BlockSpec(memory_space=pltpu.HBM)

COVER = pl.CostEstimate(flops=1 << 34, bytes_accessed=1 << 16, transcendentals=0)


def call(body, name, mib, in_specs, out_shape, scratch=(), cost=None):
    return pl.pallas_call(
        body,
        in_specs=in_specs,
        out_specs=jax.tree.map(lambda _: VMEM, out_shape),
        out_shape=out_shape,
        scratch_shapes=scratch,
        cost_estimate=cost,
        compiler_params=pltpu.CompilerParams(vmem_limit_bytes=mib << 20),
        name=name,
    )


def dot(a, b, dims=((1,), (0,))):
    return lax.dot_general(a, b, (dims, ((), ())), preferred_element_type=f32)


def in_hbm(array):
    return pltpu.with_memory_space_constraint(array, pltpu.HBM)


def iota(shape, dim):
    return lax.broadcasted_iota(i32, shape, dim)


def placed_from(ids, first, expert_count):
    return jnp.where(ids >= first, ids - first, ids + (expert_count - first))


def slot_ranks(ids, expert_count):
    top, rows = ids.shape
    experts = iota((expert_count, rows), 0)
    named = ids[0:1] == experts
    for k in range(1, top):
        named = named | (ids[k : k + 1] == experts)
    named = jnp.where(named, 1.0, 0.0)
    earlier = jnp.where(iota((rows, rows), 0) < iota((rows, rows), 1), 1.0, 0.0)
    return named, dot(named.astype(bf16), earlier.astype(bf16))


def pack_body(ids_hbm, hidden_hbm, out_ref, ids_ref, hidden_ref, sems, *, first, expert_count, capacity):
    ids_copy = pltpu.make_async_copy(ids_hbm, ids_ref, sems.at[0])
    hidden_copy = pltpu.make_async_copy(hidden_hbm, hidden_ref, sems.at[1])
    ids_copy.start()
    hidden_copy.start()
    slots = expert_count * capacity
    spread = iota((slots, expert_count), 0) // capacity == iota((slots, expert_count), 1)
    spread = jnp.where(spread, 1.0, 0.0).astype(bf16)
    ids_copy.wait()
    named, rank = slot_ranks(placed_from(ids_ref[...], first, expert_count), expert_count)
    code = jnp.where(named > 0, rank, -1.0).astype(bf16)
    wanted = dot(spread, code)
    own = (iota(wanted.shape, 0) % capacity).astype(f32)
    placing = jnp.where(wanted == own, 1.0, 0.0).astype(bf16)
    hidden_copy.wait()
    out_ref[...] = dot(placing, hidden_ref[...]).astype(bf16)


def pack(ids, hidden, first, expert_count, capacity):
    body = functools.partial(pack_body, first=first, expert_count=expert_count, capacity=capacity)
    out = jax.ShapeDtypeStruct((expert_count * capacity, hidden.shape[1]), bf16)
    scratch = [pltpu.VMEM(ids.shape, i32), pltpu.VMEM(hidden.shape, bf16), pltpu.SemaphoreType.DMA((2,))]
    return call(body, "pack", 4, [HBM] * 2, out, scratch, COVER)(in_hbm(ids), in_hbm(hidden))


def own_body(tp_ref, own_ref, gate_ref, up_hbm, down_hbm, gate_out, up_out, up_rest, down_send, up_ref, sems, *, tile):
    half = own_ref.shape[1]
    units = gate_out.shape[1]
    mine = pl.ds(pl.multiple_of(tp_ref[0] * half, half), half)
    theirs = pl.ds(pl.multiple_of((1 - tp_ref[0]) * half, half), half)
    here = pltpu.make_async_copy(up_hbm.at[0, mine, :], up_ref, sems.at[0])
    rest = pltpu.make_async_copy(up_hbm.at[0, theirs, :], up_rest, sems.at[1])
    down = pltpu.make_async_copy(down_hbm.at[0, :, theirs], down_send, sems.at[2])
    here.start()
    own = own_ref[...]
    for start in range(0, units, tile):
        if start == tile:
            rest.start()
            down.start()
        at = slice(start, start + tile)
        gate_out[:, at] = dot(own, gate_ref[0, mine, at])
    here.wait()
    for start in range(0, units, tile):
        at = slice(start, start + tile)
        up_out[:, at] = dot(own, up_ref[:, at])
    rest.wait()
    down.wait()


def own_part(tp, own, gate, up, down, tile=256):
    rows, half = own.shape
    units = gate.shape[2]
    cost = pl.CostEstimate(flops=4 * rows * units * half, bytes_accessed=4 * units * half, transcendentals=0)
    shape = jax.ShapeDtypeStruct
    out = [shape((rows, units), f32)] * 2 + [shape((half, units), bf16), shape((units, half), bf16)]
    scratch = [pltpu.VMEM((half, units), bf16), pltpu.SemaphoreType.DMA((3,))]
    body = functools.partial(own_body, tile=tile)
    specs = [SMEM, VMEM, VMEM, HBM, HBM]
    return call(body, "own_part", 8, specs, out, scratch, cost)(tp, own, gate, in_hbm(up), in_hbm(down))


def hidden_body(tp_ref, other_ref, gate_in, up_in, gate_ref, up_ref, down_ref, act_ref, send_ref, *, tile):
    half = other_ref.shape[1]
    theirs = pl.ds(pl.multiple_of((1 - tp_ref[0]) * half, half), half)
    other = other_ref[...]
    for start in range(0, gate_ref.shape[2], tile):
        at = slice(start, start + tile)
        gate = gate_in[:, at] + dot(other, gate_ref[0, theirs, at])
        up = up_in[:, at] + dot(other, up_ref[:, at])
        act_ref[:, at] = (gate / (1.0 + jnp.exp(-gate)) * up).astype(bf16)
    send_ref[...] = dot(act_ref[...], down_ref[...]).astype(bf16)


def hidden_part(tp, other, gate_in, up_in, gate, up_rest, down_send, tile=256):
    rows, half = other.shape
    units = gate.shape[2]
    cost = pl.CostEstimate(flops=6 * rows * units * half, bytes_accessed=6 * units * half, transcendentals=rows * units)
    out = [jax.ShapeDtypeStruct((rows, units), bf16), jax.ShapeDtypeStruct((rows, half), bf16)]
    body = functools.partial(hidden_body, tile=tile)
    return call(body, "hidden_part", 8, [SMEM] + [VMEM] * 6, out, cost=cost)(
        tp, other, gate_in, up_in, gate, up_rest, down_send
    )


def keep_body(tp_ref, act_ref, down_ref, out_ref):
    half = out_ref.shape[1]
    mine = pl.ds(pl.multiple_of(tp_ref[0] * half, half), half)
    out_ref[...] = dot(act_ref[...], down_ref[0, :, mine]).astype(bf16)


def keep_part(tp, act, down, half):
    rows, units = act.shape
    cost = pl.CostEstimate(flops=2 * rows * units * half, bytes_accessed=2 * units * half, transcendentals=0)
    out = jax.ShapeDtypeStruct((rows, half), bf16)
    return call(keep_body, "keep_part", 8, [SMEM] + [VMEM] * 2, out, cost=cost)(tp, act, down)


def weigh_body(ids_ref, weight_ref, high_ref, low_ref, *, first, expert_count, capacity):
    ids = placed_from(ids_ref[...], first, expert_count)
    top, rows = ids.shape
    _, rank = slot_ranks(ids, expert_count)
    experts = iota((expert_count, rows), 0)
    places = iota((expert_count * capacity, rows), 0)
    weights = jnp.zeros(places.shape, f32)
    for k in range(top):
        row = ids[k : k + 1]
        at = jnp.sum(jnp.where(row == experts, rank, 0.0), axis=0, keepdims=True).astype(i32)
        weights += jnp.where(row * capacity + at == places, weight_ref[k : k + 1], 0.0)
    high = weights.astype(bf16)
    high_ref[...] = high
    low_ref[...] = (weights - high.astype(f32)).astype(bf16)


def weigh(ids, weights, first, expert_count, capacity):
    body = functools.partial(weigh_body, first=first, expert_count=expert_count, capacity=capacity)
    out = [jax.ShapeDtypeStruct((expert_count * capacity, ids.shape[1]), bf16)] * 2
    return call(body, "weigh", 4, [VMEM] * 2, out)(ids, weights)


def combine_body(high_ref, low_ref, back_ref, out_ref, square_ref):
    back = back_ref[...]
    over = ((0,), (0,))
    combined = dot(high_ref[...], back, over) + dot(low_ref[...], back, over)
    out_ref[...] = combined
    square_ref[...] = jnp.broadcast_to(jnp.sum(combined * combined, axis=1, keepdims=True), square_ref.shape)


def combine(high, low, back):
    rows = high.shape[1]
    out = [jax.ShapeDtypeStruct((rows, back.shape[1]), f32), jax.ShapeDtypeStruct((rows, 128), f32)]
    return call(combine_body, "combine", 4, [VMEM] * 3, out)(high, low, back)


def norm_body(combined_ref, square_ref, other_ref, gain_ref, out_ref, *, width):
    total = (square_ref[...] + other_ref[...])[:, 0:1]
    out_ref[...] = (combined_ref[...] * lax.rsqrt(total / width + norm_eps) * gain_ref[...]).astype(bf16)


def norm(combined, squares, others, gain, width):
    body = functools.partial(norm_body, width=width)
    out = jax.ShapeDtypeStruct(combined.shape, bf16)
    return call(body, "norm", 4, [VMEM] * 4, out)(combined, squares, others, gain.reshape(1, -1))


def shards(hidden_state, expert_ids, route_weight, gate_matrix, up_matrix, down_matrix, norm_gain):
    tok_count, top_count = expert_ids.shape
    half = hidden_state.shape[1]
    experts = lax.axis_size("ep")
    capacity = max(2, 2 * tok_count * top_count // experts)
    tp = lax.axis_index("tp").reshape(1)
    ids, weights = expert_ids.T, route_weight.T
    swap = lambda a: lax.ppermute(a, "tp", [(0, 1), (1, 0)])
    first = experts - experts // 16
    members = [[(first + place) % experts for place in range(experts)]]
    exchange = lambda a: lax.all_to_all(
        a.reshape(experts, capacity, half), "ep", 0, 0, tiled=True, axis_index_groups=members
    ).reshape(experts * capacity, half)
    own = exchange(pack(ids, hidden_state, first, experts, capacity))
    gate_part, up_part, up_rest, down_send = own_part(tp, own, gate_matrix, up_matrix, down_matrix)
    act, send = hidden_part(tp, swap(own), gate_part, up_part, gate_matrix, up_rest, down_send)
    got = swap(send)
    kept = keep_part(tp, act, down_matrix, half)
    kept, high, low = lax.optimization_barrier((kept, *weigh(ids, weights, first, experts, capacity)))
    answers = (kept.astype(f32) + got.astype(f32)).astype(bf16)
    combined, squares = combine(high, low, exchange(answers))
    return norm(combined, squares, swap(squares), norm_gain, half * lax.axis_size("tp"))


def solution(mesh):
    placed = (
        P(("grp", "ep"), "tp"),
        P(("grp", "ep"), None),
        P(("grp", "ep"), None),
        P("ep", None, "tp"),
        P("ep", None, "tp"),
        P("ep", "tp", None),
        P("tp"),
    )
    return jax.shard_map(
        shards, mesh=mesh, in_specs=placed, out_specs=P(("grp", "ep"), "tp"), check_vma=False
    )
```

```python
import functools

import jax
import jax.numpy as jnp
from jax import lax
from jax.experimental import pallas as pl
from jax.experimental.pallas import tpu as pltpu
from jax.sharding import PartitionSpec as P

norm_eps = 1e-05
f32, bf16, i32 = jnp.float32, jnp.bfloat16, jnp.int32
VMEM = pl.BlockSpec(memory_space=pltpu.VMEM)
SMEM = pl.BlockSpec(memory_space=pltpu.SMEM)
HBM = pl.BlockSpec(memory_space=pltpu.HBM)

COVER = pl.CostEstimate(flops=1 << 34, bytes_accessed=1 << 16, transcendentals=0)


def call(body, name, mib, in_specs, out_shape, scratch=(), cost=None):
    return pl.pallas_call(
        body,
        in_specs=in_specs,
        out_specs=jax.tree.map(lambda _: VMEM, out_shape),
        out_shape=out_shape,
        scratch_shapes=scratch,
        cost_estimate=cost,
        compiler_params=pltpu.CompilerParams(vmem_limit_bytes=mib << 20),
        name=name,
    )


def dot(a, b, dims=((1,), (0,))):
    return lax.dot_general(a, b, (dims, ((), ())), preferred_element_type=f32)


def in_hbm(array):
    return pltpu.with_memory_space_constraint(array, pltpu.HBM)


def iota(shape, dim):
    return lax.broadcasted_iota(i32, shape, dim)


def placed_from(ids, first, expert_count):
    return jnp.where(ids >= first, ids - first, ids + (expert_count - first))


def slot_ranks(ids, expert_count):
    top, rows = ids.shape
    experts = iota((expert_count, rows), 0)
    named = ids[0:1] == experts
    for k in range(1, top):
        named = named | (ids[k : k + 1] == experts)
    named = jnp.where(named, 1.0, 0.0)
    earlier = jnp.where(iota((rows, rows), 0) < iota((rows, rows), 1), 1.0, 0.0)
    return named, dot(named.astype(bf16), earlier.astype(bf16))


def pack_body(ids_hbm, hidden_hbm, out_ref, ids_ref, hidden_ref, sems, *, first, expert_count, capacity):
    ids_copy = pltpu.make_async_copy(ids_hbm, ids_ref, sems.at[0])
    hidden_copy = pltpu.make_async_copy(hidden_hbm, hidden_ref, sems.at[1])
    ids_copy.start()
    hidden_copy.start()
    slots = expert_count * capacity
    spread = iota((slots, expert_count), 0) // capacity == iota((slots, expert_count), 1)
    spread = jnp.where(spread, 1.0, 0.0).astype(bf16)
    ids_copy.wait()
    named, rank = slot_ranks(placed_from(ids_ref[...], first, expert_count), expert_count)
    code = jnp.where(named > 0, rank, -1.0).astype(bf16)
    wanted = dot(spread, code)
    own = (iota(wanted.shape, 0) % capacity).astype(f32)
    placing = jnp.where(wanted == own, 1.0, 0.0).astype(bf16)
    hidden_copy.wait()
    out_ref[...] = dot(placing, hidden_ref[...]).astype(bf16)


def pack(ids, hidden, first, expert_count, capacity):
    body = functools.partial(pack_body, first=first, expert_count=expert_count, capacity=capacity)
    out = jax.ShapeDtypeStruct((expert_count * capacity, hidden.shape[1]), bf16)
    scratch = [pltpu.VMEM(ids.shape, i32), pltpu.VMEM(hidden.shape, bf16), pltpu.SemaphoreType.DMA((2,))]
    return call(body, "pack", 4, [HBM] * 2, out, scratch, COVER)(in_hbm(ids), in_hbm(hidden))


def own_body(tp_ref, own_ref, gate_ref, up_hbm, down_hbm, gate_out, up_out, up_rest, down_send, up_ref, sems, *, tile):
    half = own_ref.shape[1]
    units = gate_out.shape[1]
    mine = pl.ds(pl.multiple_of(tp_ref[0] * half, half), half)
    theirs = pl.ds(pl.multiple_of((1 - tp_ref[0]) * half, half), half)
    here = pltpu.make_async_copy(up_hbm.at[0, mine, :], up_ref, sems.at[0])
    rest = pltpu.make_async_copy(up_hbm.at[0, theirs, :], up_rest, sems.at[1])
    down = pltpu.make_async_copy(down_hbm.at[0, :, theirs], down_send, sems.at[2])
    here.start()
    own = own_ref[...]
    for start in range(0, units, tile):
        if start == tile:
            rest.start()
            down.start()
        at = slice(start, start + tile)
        gate_out[:, at] = dot(own, gate_ref[0, mine, at])
    here.wait()
    for start in range(0, units, tile):
        at = slice(start, start + tile)
        up_out[:, at] = dot(own, up_ref[:, at])
    rest.wait()
    down.wait()


def own_part(tp, own, gate, up, down, tile=256):
    rows, half = own.shape
    units = gate.shape[2]
    cost = pl.CostEstimate(flops=4 * rows * units * half, bytes_accessed=4 * units * half, transcendentals=0)
    shape = jax.ShapeDtypeStruct
    out = [shape((rows, units), f32)] * 2 + [shape((half, units), bf16), shape((units, half), bf16)]
    scratch = [pltpu.VMEM((half, units), bf16), pltpu.SemaphoreType.DMA((3,))]
    body = functools.partial(own_body, tile=tile)
    specs = [SMEM, VMEM, VMEM, HBM, HBM]
    return call(body, "own_part", 8, specs, out, scratch, cost)(tp, own, gate, in_hbm(up), in_hbm(down))


def hidden_body(tp_ref, other_ref, gate_in, up_in, gate_ref, up_ref, down_ref, act_ref, send_ref, *, tile):
    half = other_ref.shape[1]
    theirs = pl.ds(pl.multiple_of((1 - tp_ref[0]) * half, half), half)
    other = other_ref[...]
    for start in range(0, gate_ref.shape[2], tile):
        at = slice(start, start + tile)
        gate = gate_in[:, at] + dot(other, gate_ref[0, theirs, at])
        up = up_in[:, at] + dot(other, up_ref[:, at])
        act_ref[:, at] = (gate / (1.0 + jnp.exp(-gate)) * up).astype(bf16)
    send_ref[...] = dot(act_ref[...], down_ref[...]).astype(bf16)


def hidden_part(tp, other, gate_in, up_in, gate, up_rest, down_send, tile=256):
    rows, half = other.shape
    units = gate.shape[2]
    cost = pl.CostEstimate(flops=6 * rows * units * half, bytes_accessed=6 * units * half, transcendentals=rows * units)
    out = [jax.ShapeDtypeStruct((rows, units), bf16), jax.ShapeDtypeStruct((rows, half), bf16)]
    body = functools.partial(hidden_body, tile=tile)
    return call(body, "hidden_part", 8, [SMEM] + [VMEM] * 6, out, cost=cost)(
        tp, other, gate_in, up_in, gate, up_rest, down_send
    )


def keep_body(tp_ref, act_ref, down_ref, out_ref):
    half = out_ref.shape[1]
    mine = pl.ds(pl.multiple_of(tp_ref[0] * half, half), half)
    out_ref[...] = dot(act_ref[...], down_ref[0, :, mine]).astype(bf16)


def keep_part(tp, act, down, half):
    rows, units = act.shape
    cost = pl.CostEstimate(flops=2 * rows * units * half, bytes_accessed=2 * units * half, transcendentals=0)
    out = jax.ShapeDtypeStruct((rows, half), bf16)
    return call(keep_body, "keep_part", 8, [SMEM] + [VMEM] * 2, out, cost=cost)(tp, act, down)


def add_body(kept_ref, got_ref, out_ref, *, turn):
    rows = out_ref.shape[0]
    for start, end, to in ((turn, rows, 0), (0, turn, rows - turn)):
        total = kept_ref[start:end].astype(f32) + got_ref[start:end].astype(f32)
        out_ref[to : to + end - start] = total.astype(bf16)


def add_turned(kept, got, turn):
    body = functools.partial(add_body, turn=turn)
    return call(body, "add_turned", 4, [VMEM] * 2, jax.ShapeDtypeStruct(kept.shape, bf16))(kept, got)


def weigh_body(ids_ref, weight_ref, high_ref, low_ref, *, first, expert_count, capacity):
    ids = placed_from(ids_ref[...], first, expert_count)
    top, rows = ids.shape
    _, rank = slot_ranks(ids, expert_count)
    experts = iota((expert_count, rows), 0)
    places = iota((expert_count * capacity, rows), 0)
    weights = jnp.zeros(places.shape, f32)
    for k in range(top):
        row = ids[k : k + 1]
        at = jnp.sum(jnp.where(row == experts, rank, 0.0), axis=0, keepdims=True).astype(i32)
        weights += jnp.where(row * capacity + at == places, weight_ref[k : k + 1], 0.0)
    high = weights.astype(bf16)
    high_ref[...] = high
    low_ref[...] = (weights - high.astype(f32)).astype(bf16)


def weigh(ids, weights, first, expert_count, capacity):
    body = functools.partial(weigh_body, first=first, expert_count=expert_count, capacity=capacity)
    out = [jax.ShapeDtypeStruct((expert_count * capacity, ids.shape[1]), bf16)] * 2
    return call(body, "weigh", 4, [VMEM] * 2, out)(ids, weights)


def combine_body(high_ref, low_ref, back_ref, out_ref, square_ref):
    back = back_ref[...]
    over = ((0,), (0,))
    combined = dot(high_ref[...], back, over) + dot(low_ref[...], back, over)
    out_ref[...] = combined
    square_ref[...] = jnp.broadcast_to(jnp.sum(combined * combined, axis=1, keepdims=True), square_ref.shape)


def combine(high, low, back):
    rows = high.shape[1]
    out = [jax.ShapeDtypeStruct((rows, back.shape[1]), f32), jax.ShapeDtypeStruct((rows, 128), f32)]
    return call(combine_body, "combine", 4, [VMEM] * 3, out)(high, low, back)


def norm_body(combined_ref, square_ref, other_ref, gain_ref, out_ref, *, width):
    total = (square_ref[...] + other_ref[...])[:, 0:1]
    out_ref[...] = (combined_ref[...] * lax.rsqrt(total / width + norm_eps) * gain_ref[...]).astype(bf16)


def norm(combined, squares, others, gain, width):
    body = functools.partial(norm_body, width=width)
    out = jax.ShapeDtypeStruct(combined.shape, bf16)
    return call(body, "norm", 4, [VMEM] * 4, out)(combined, squares, others, gain.reshape(1, -1))


def shards(hidden_state, expert_ids, route_weight, gate_matrix, up_matrix, down_matrix, norm_gain):
    tok_count, top_count = expert_ids.shape
    half = hidden_state.shape[1]
    experts = lax.axis_size("ep")
    capacity = max(2, 2 * tok_count * top_count // experts)
    tp = lax.axis_index("tp").reshape(1)
    ids, weights = expert_ids.T, route_weight.T
    swap = lambda a: lax.ppermute(a, "tp", [(0, 1), (1, 0)])
    first = experts - experts // 16
    back = experts - experts // 8
    exchange = lambda a, first: lax.all_to_all(
        a.reshape(experts, capacity, half),
        "ep",
        0,
        0,
        tiled=True,
        axis_index_groups=[[(first + place) % experts for place in range(experts)]],
    ).reshape(experts * capacity, half)
    own = exchange(pack(ids, hidden_state, first, experts, capacity), first)
    gate_part, up_part, up_rest, down_send = own_part(tp, own, gate_matrix, up_matrix, down_matrix)
    act, send = hidden_part(tp, swap(own), gate_part, up_part, gate_matrix, up_rest, down_send)
    got = swap(send)
    kept = keep_part(tp, act, down_matrix, half)
    kept, high, low = lax.optimization_barrier((kept, *weigh(ids, weights, back, experts, capacity)))
    answers = add_turned(kept, got, (back - first) % experts * capacity)
    combined, squares = combine(high, low, exchange(answers, back))
    return norm(combined, squares, swap(squares), norm_gain, half * lax.axis_size("tp"))


def solution(mesh):
    placed = (
        P(("grp", "ep"), "tp"),
        P(("grp", "ep"), None),
        P(("grp", "ep"), None),
        P("ep", None, "tp"),
        P("ep", None, "tp"),
        P("ep", "tp", None),
        P("tp"),
    )
    return jax.shard_map(
        shards, mesh=mesh, in_specs=placed, out_specs=P(("grp", "ep"), "tp"), check_vma=False
    )
```

```python
import functools

import jax
import jax.numpy as jnp
from jax import lax
from jax.experimental import pallas as pl
from jax.experimental.pallas import tpu as pltpu
from jax.sharding import PartitionSpec as P

norm_eps = 1e-05
f32, bf16, i32 = jnp.float32, jnp.bfloat16, jnp.int32
VMEM = pl.BlockSpec(memory_space=pltpu.VMEM)
SMEM = pl.BlockSpec(memory_space=pltpu.SMEM)
HBM = pl.BlockSpec(memory_space=pltpu.HBM)

COVER = pl.CostEstimate(flops=1 << 34, bytes_accessed=1 << 16, transcendentals=0)


def call(body, name, mib, in_specs, out_shape, scratch=(), cost=None):
    return pl.pallas_call(
        body,
        in_specs=in_specs,
        out_specs=jax.tree.map(lambda _: VMEM, out_shape),
        out_shape=out_shape,
        scratch_shapes=scratch,
        cost_estimate=cost,
        compiler_params=pltpu.CompilerParams(vmem_limit_bytes=mib << 20),
        name=name,
    )


def dot(a, b, dims=((1,), (0,))):
    return lax.dot_general(a, b, (dims, ((), ())), preferred_element_type=f32)


def in_hbm(array):
    return pltpu.with_memory_space_constraint(array, pltpu.HBM)


def iota(shape, dim):
    return lax.broadcasted_iota(i32, shape, dim)


def placed_from(ids, first, expert_count):
    return jnp.where(ids >= first, ids - first, ids + (expert_count - first))


def slot_ranks(ids, expert_count):
    top, rows = ids.shape
    experts = iota((expert_count, rows), 0)
    named = ids[0:1] == experts
    for k in range(1, top):
        named = named | (ids[k : k + 1] == experts)
    named = jnp.where(named, 1.0, 0.0)
    earlier = jnp.where(iota((rows, rows), 0) < iota((rows, rows), 1), 1.0, 0.0)
    return named, dot(named.astype(bf16), earlier.astype(bf16))


def pack_body(ids_hbm, hidden_hbm, out_ref, ids_ref, hidden_ref, sems, *, first, expert_count, capacity):
    ids_copy = pltpu.make_async_copy(ids_hbm, ids_ref, sems.at[0])
    hidden_copy = pltpu.make_async_copy(hidden_hbm, hidden_ref, sems.at[1])
    ids_copy.start()
    hidden_copy.start()
    slots = expert_count * capacity
    spread = iota((slots, expert_count), 0) // capacity == iota((slots, expert_count), 1)
    spread = jnp.where(spread, 1.0, 0.0).astype(bf16)
    ids_copy.wait()
    named, rank = slot_ranks(placed_from(ids_ref[...], first, expert_count), expert_count)
    code = jnp.where(named > 0, rank, -1.0).astype(bf16)
    wanted = dot(spread, code)
    own = (iota(wanted.shape, 0) % capacity).astype(f32)
    placing = jnp.where(wanted == own, 1.0, 0.0).astype(bf16)
    hidden_copy.wait()
    out_ref[...] = dot(placing, hidden_ref[...]).astype(bf16)


def pack(ids, hidden, first, expert_count, capacity):
    body = functools.partial(pack_body, first=first, expert_count=expert_count, capacity=capacity)
    out = jax.ShapeDtypeStruct((expert_count * capacity, hidden.shape[1]), bf16)
    scratch = [pltpu.VMEM(ids.shape, i32), pltpu.VMEM(hidden.shape, bf16), pltpu.SemaphoreType.DMA((2,))]
    return call(body, "pack", 4, [HBM] * 2, out, scratch, COVER)(in_hbm(ids), in_hbm(hidden))


def own_body(tp_ref, own_ref, gate_ref, up_hbm, down_hbm, gate_out, up_out, up_rest, down_send, up_ref, sems, *, tile):
    half = own_ref.shape[1]
    units = gate_out.shape[1]
    mine = pl.ds(pl.multiple_of(tp_ref[0] * half, half), half)
    theirs = pl.ds(pl.multiple_of((1 - tp_ref[0]) * half, half), half)
    here = pltpu.make_async_copy(up_hbm.at[0, mine, :], up_ref, sems.at[0])
    rest = pltpu.make_async_copy(up_hbm.at[0, theirs, :], up_rest, sems.at[1])
    down = pltpu.make_async_copy(down_hbm.at[0, :, theirs], down_send, sems.at[2])
    here.start()
    own = own_ref[...]
    for start in range(0, units, tile):
        if start == tile:
            rest.start()
            down.start()
        at = slice(start, start + tile)
        gate_out[:, at] = dot(own, gate_ref[0, mine, at])
    here.wait()
    for start in range(0, units, tile):
        at = slice(start, start + tile)
        up_out[:, at] = dot(own, up_ref[:, at])
    rest.wait()
    down.wait()


def own_part(tp, own, gate, up, down, tile=256):
    rows, half = own.shape
    units = gate.shape[2]
    cost = pl.CostEstimate(flops=4 * rows * units * half, bytes_accessed=4 * units * half, transcendentals=0)
    shape = jax.ShapeDtypeStruct
    out = [shape((rows, units), f32)] * 2 + [shape((half, units), bf16), shape((units, half), bf16)]
    scratch = [pltpu.VMEM((half, units), bf16), pltpu.SemaphoreType.DMA((3,))]
    body = functools.partial(own_body, tile=tile)
    specs = [SMEM, VMEM, VMEM, HBM, HBM]
    return call(body, "own_part", 8, specs, out, scratch, cost)(tp, own, gate, in_hbm(up), in_hbm(down))


def hidden_body(tp_ref, other_ref, gate_in, up_in, gate_ref, up_ref, down_ref, act_ref, send_ref, *, tile):
    half = other_ref.shape[1]
    theirs = pl.ds(pl.multiple_of((1 - tp_ref[0]) * half, half), half)
    other = other_ref[...]
    for start in range(0, gate_ref.shape[2], tile):
        at = slice(start, start + tile)
        gate = gate_in[:, at] + dot(other, gate_ref[0, theirs, at])
        up = up_in[:, at] + dot(other, up_ref[:, at])
        act_ref[:, at] = (gate / (1.0 + jnp.exp(-gate)) * up).astype(bf16)
    send_ref[...] = dot(act_ref[...], down_ref[...]).astype(bf16)


def hidden_part(tp, other, gate_in, up_in, gate, up_rest, down_send, tile=256):
    rows, half = other.shape
    units = gate.shape[2]
    cost = pl.CostEstimate(flops=6 * rows * units * half, bytes_accessed=6 * units * half, transcendentals=rows * units)
    out = [jax.ShapeDtypeStruct((rows, units), bf16), jax.ShapeDtypeStruct((rows, half), bf16)]
    body = functools.partial(hidden_body, tile=tile)
    return call(body, "hidden_part", 8, [SMEM] + [VMEM] * 6, out, cost=cost)(
        tp, other, gate_in, up_in, gate, up_rest, down_send
    )


def keep_body(tp_ref, act_ref, down_ref, out_ref):
    half = out_ref.shape[1]
    mine = pl.ds(pl.multiple_of(tp_ref[0] * half, half), half)
    out_ref[...] = dot(act_ref[...], down_ref[0, :, mine]).astype(bf16)


def keep_part(tp, act, down, half):
    rows, units = act.shape
    cost = pl.CostEstimate(flops=2 * rows * units * half, bytes_accessed=2 * units * half, transcendentals=0)
    out = jax.ShapeDtypeStruct((rows, half), bf16)
    return call(keep_body, "keep_part", 8, [SMEM] + [VMEM] * 2, out, cost=cost)(tp, act, down)


def weigh_body(ids_ref, weight_ref, out_ref, *, first, expert_count, capacity):
    ids = placed_from(ids_ref[...], first, expert_count)
    top, rows = ids.shape
    _, rank = slot_ranks(ids, expert_count)
    experts = iota((expert_count, rows), 0)
    places = iota((expert_count * capacity, rows), 0)
    weights = jnp.zeros(places.shape, f32)
    for k in range(top):
        row = ids[k : k + 1]
        at = jnp.sum(jnp.where(row == experts, rank, 0.0), axis=0, keepdims=True).astype(i32)
        weights += jnp.where(row * capacity + at == places, weight_ref[k : k + 1], 0.0)
    high = weights.astype(bf16)
    out_ref[:, :rows] = high
    out_ref[:, rows:] = (weights - high.astype(f32)).astype(bf16)


def weigh(ids, weights, first, expert_count, capacity):
    body = functools.partial(weigh_body, first=first, expert_count=expert_count, capacity=capacity)
    out = jax.ShapeDtypeStruct((expert_count * capacity, 2 * ids.shape[1]), bf16)
    return call(body, "weigh", 4, [VMEM] * 2, out)(ids, weights)


def combine_body(terms_ref, back_ref, out_ref, square_ref):
    both = dot(terms_ref[...], back_ref[...], ((0,), (0,)))
    rows = out_ref.shape[0]
    combined = both[:rows] + both[rows:]
    out_ref[...] = combined
    square_ref[...] = jnp.broadcast_to(jnp.sum(combined * combined, axis=1, keepdims=True), square_ref.shape)


def combine(terms, back):
    rows = terms.shape[1] // 2
    out = [jax.ShapeDtypeStruct((rows, back.shape[1]), f32), jax.ShapeDtypeStruct((rows, 128), f32)]
    return call(combine_body, "combine", 4, [VMEM] * 2, out)(terms, back)


def norm_body(combined_ref, square_ref, other_ref, gain_ref, out_ref, *, width):
    total = (square_ref[...] + other_ref[...])[:, 0:1]
    out_ref[...] = (combined_ref[...] * lax.rsqrt(total / width + norm_eps) * gain_ref[...]).astype(bf16)


def norm(combined, squares, others, gain, width):
    body = functools.partial(norm_body, width=width)
    out = jax.ShapeDtypeStruct(combined.shape, bf16)
    return call(body, "norm", 4, [VMEM] * 4, out)(combined, squares, others, gain.reshape(1, -1))


def shards(hidden_state, expert_ids, route_weight, gate_matrix, up_matrix, down_matrix, norm_gain):
    tok_count, top_count = expert_ids.shape
    half = hidden_state.shape[1]
    experts = lax.axis_size("ep")
    capacity = max(2, 2 * tok_count * top_count // experts)
    tp = lax.axis_index("tp").reshape(1)
    ids, weights = expert_ids.T, route_weight.T
    swap = lambda a: lax.ppermute(a, "tp", [(0, 1), (1, 0)])
    first = experts - experts // 16
    members = [[(first + place) % experts for place in range(experts)]]
    exchange = lambda a: lax.all_to_all(
        a.reshape(experts, capacity, half), "ep", 0, 0, tiled=True, axis_index_groups=members
    ).reshape(experts * capacity, half)
    own = exchange(pack(ids, hidden_state, first, experts, capacity))
    gate_part, up_part, up_rest, down_send = own_part(tp, own, gate_matrix, up_matrix, down_matrix)
    act, send = hidden_part(tp, swap(own), gate_part, up_part, gate_matrix, up_rest, down_send)
    got = swap(send)
    kept = keep_part(tp, act, down_matrix, half)
    kept, terms = lax.optimization_barrier((kept, weigh(ids, weights, first, experts, capacity)))
    answers = (kept.astype(f32) + got.astype(f32)).astype(bf16)
    combined, squares = combine(terms, exchange(answers))
    return norm(combined, squares, swap(squares), norm_gain, half * lax.axis_size("tp"))


def solution(mesh):
    placed = (
        P(("grp", "ep"), "tp"),
        P(("grp", "ep"), None),
        P(("grp", "ep"), None),
        P("ep", None, "tp"),
        P("ep", None, "tp"),
        P("ep", "tp", None),
        P("tp"),
    )
    return jax.shard_map(
        shards, mesh=mesh, in_specs=placed, out_specs=P(("grp", "ep"), "tp"), check_vma=False
    )
```
